512 devices in a mesh: grp: 2 (over y), ep: 32 (over z, core), tp: 8 (over x).
Axes of the slice: x: 8, y: 2, z: 16, core: 2. Of those that a mesh axis runs over, the one named last changes fastest.
The devices are a block of a 8x8x16 slice.
Arguments:
- tokens: bfloat16 [4096, 2048], P(('grp', 'ep')), parts along dimension 0, may hold values from -6 to 6
- norm_gain: float32 [2048], replicated, may hold values from 0.1 to 1.9
- routes: int32 [4096, 6], P(('grp', 'ep')), parts along dimension 0, may hold values from 0 to 31, all different within a row; in each aligned block of 64 rows (0 to 63, 64 to 127, ...) at most 24 rows name the same one
- route_weights: float32 [4096, 6], P(('grp', 'ep')), parts along dimension 0, may hold values from 0.05 to 1
- w_gate: bfloat16 [32, 2048, 2048], P('ep', None, 'tp'), may hold values from -0.125 to 0.125
- w_up: bfloat16 [32, 2048, 2048], P('ep', None, 'tp'), may hold values from -0.125 to 0.125
- w_down: bfloat16 [32, 2048, 2048], P('ep', 'tp'), may hold values from -4 to 4
- final_gain: float32 [2048], P('tp'), may hold values from 0.1 to 1.9
Outputs:
- mixed_out: bfloat16 [4096, 2048], P(('grp', 'ep'), 'tp'), parts along dimension 0
The draws below stay inside these ranges and needn't reach their ends.
There are 2 independent parts, one for each index of `grp`. The reference program is written for one: setup_inputs(seed, part) draws one part's arguments, and reference() takes and returns one part's arrays. A program takes and returns all parts, laid end to end along the dimension named above; an argument that names none is the same for every part. Nothing has to cross between parts.
Inputs may be any that keep to these rules, and one draw needn't show every extreme that they name: `routes`: each row names 6 different experts; within the rows of one index of ep no expert is named by more than 24 rows, and in every draw some expert is named by exactly 24 rows of some index.
All inputs are finite; a program needn't handle non-finite values.
Results may differ from the reference program's by a relative error of at most 0.015.
Values may be sent and summed in bfloat16 or wider, within the bound.
A program may use at most 64 MiB of HBM per device.

```python
import math
import jax
import jax.numpy as jnp
import numpy as np
from jax import lax

D = 2048
FF = 2048
TOP_K = 6
TOK_DEV = 64
EXPERTS = 32
CAP = 24
TOKENS = 2048
N_EP = 32
N_TP = 8


def draw_w_down(key, part):
    key_values, key_columns = jax.random.split(key)
    columns = jnp.arange(D, dtype=jnp.float32) / D
    roughness = jax.random.uniform(key_columns, (D,), jnp.float32, 0.5, 1.5)
    values = jnp.clip(jax.random.normal(key_values, (EXPERTS, FF, D), jnp.float32), -5.0, 5.0)
    column_scale = jnp.exp(columns * jnp.log(10.0)) * roughness
    scaled = values * column_scale[None, None, :] * FF ** (-0.5) / 3.0
    return scaled.astype(jnp.bfloat16)


def block_scale(own_key, shape, cuts, smallest, high):
    loudness, own = 1.0, jax.random.fold_in(own_key, 6)
    for position, blocks in cuts:
        steps = jnp.exp(jax.random.uniform(jax.random.fold_in(own, position), (blocks,), jnp.float32, smallest / len(cuts), high / len(cuts)))
        loudness = loudness * jnp.repeat(steps, shape[position] // blocks).reshape([-1 if axis == position else 1 for axis in range(len(shape))])
    return loudness


def deal_out(key, own, number, rows, count, top, reach, slope):
    order = jax.random.permutation(key, count)
    crowded, common = load_shares(count, rows * top, reach, slope, True), load_shares(count, rows * top, reach, slope, False)
    places = jnp.arange(count)

    def named(sizes, offset_by):
        used = int((sizes > 0).sum())
        fixed = max(1, used // 4)
        shifted = fixed + (places - fixed + offset_by * (used - fixed)) % max(1, count - fixed)
        return jnp.zeros((count,), jnp.int32).at[order[jnp.where(places < fixed, places, shifted)]].set(jnp.asarray(sizes, jnp.int32))

    sizes = jnp.where(number % 4 == 0, named(crowded, number // 4), named(common, number - number // 4 - 1))
    mixed = jax.random.permutation(jax.random.fold_in(own, 3), count)
    source_of, taker = mixed[0:count // 2 * 2:2], mixed[1:count // 2 * 2:2]
    margin = jnp.minimum(sizes[source_of] - 1, reach - sizes[taker]) // 2
    margin = jnp.where((source_of == order[0]) | (taker == order[0]) | (sizes[taker] == 0), 0, jnp.maximum(margin, 0))
    shifted = jax.random.randint(jax.random.fold_in(own, 4), (count // 2,), 0, 1 << 20) % (margin + 1)
    sizes = sizes.at[source_of].add(-shifted).at[taker].add(shifted)
    labels = jnp.searchsorted(jnp.cumsum(sizes), jnp.arange(rows * top), side="right").astype(jnp.int32)
    listing = labels.reshape(top, rows).T
    listing = listing[jax.random.permutation(jax.random.fold_in(own, 1), rows)]
    offset_by = jax.random.randint(jax.random.fold_in(own, 2), (rows, 1), 0, top)
    return jnp.take_along_axis(listing, (jnp.arange(top)[None, :] + offset_by) % top, axis=1)


def load_shares(number_of, total, reach, slope, full):
    weights = [(1 << 20) // math.isqrt(standing ** slope) + 1 for standing in range(1, number_of + 1)]
    largest = reach if full else min(reach, max(-(-total // number_of), total * weights[0] // sum(weights)))
    least = 1 if total - largest >= number_of - 1 else 0
    counts, surplus = [largest] + [least] * (number_of - 1), total - largest - least * (number_of - 1)
    while surplus > 0:
        candidates = [i for i in range(1, number_of) if counts[i] < largest] or [i for i in range(1, number_of) if counts[i] < reach]
        mass, left = sum([weights[i] for i in candidates]), surplus
        for i in candidates:
            more = min(reach - counts[i], max(1, left * weights[i] // mass), surplus)
            counts[i] = counts[i] + more
            surplus = surplus - more
    return np.array(counts)


def scatter_about(rng, shape, deviation, bound, cuts=(), kind=jnp.bfloat16):
    loudness = block_scale(rng, shape, cuts, -0.22, 0.18) if cuts else 1.0
    array = jax.random.normal(rng, shape, jnp.float32) * deviation * loudness
    return jnp.minimum(jnp.maximum(array, -bound), bound).astype(kind)


def setup_inputs(seed: int = 0, part: int = 0) -> dict:
    keys = jax.random.split(jax.random.key(seed), 9)
    part_splits = jax.random.split(jax.random.fold_in(keys[8], part), 9)
    tokens = scatter_about(part_splits[0], (TOKENS, D), 1.0, 6.0, ((0, 32),))
    norm_gain = jnp.clip(1.0 + 0.18 * jax.random.normal(keys[1], (D,), jnp.float32), 0.1, 1.9)
    routes_keys = jax.random.split(jax.random.fold_in(part_splits[2], 1), TOKENS // TOK_DEV)
    routes_turns = jax.random.permutation(jax.random.fold_in(part_splits[2], 3), TOKENS // TOK_DEV)
    routes = jax.vmap(lambda own, number: deal_out(jax.random.fold_in(part_splits[2], 2), own, number, TOK_DEV, EXPERTS, TOP_K, CAP, 2))(routes_keys, routes_turns).reshape((TOKENS, TOP_K))
    route_weights = jnp.clip(jnp.exp(math.log(1.0) - 2.9957323 * jax.random.uniform(part_splits[3], (TOKENS, TOP_K), jnp.float32) ** block_scale(part_splits[3], (TOKENS, TOP_K), ((0, 32),), -0.2, 0.2)), 0.05, 1.0)
    w_gate = scatter_about(keys[4], (EXPERTS, D, FF), D ** -0.5, 0.125, ((0, 32), (2, 8)))
    w_up = scatter_about(keys[5], (EXPERTS, D, FF), D ** -0.5, 0.125, ((0, 32), (2, 8)))
    w_down = draw_w_down(jax.random.fold_in(keys[8], 71), part)
    final_gain = jnp.clip(1.0 + 0.18 * jax.random.normal(keys[7], (D,), jnp.float32), 0.1, 1.9)
    return dict(tokens=tokens, norm_gain=norm_gain, routes=routes, route_weights=route_weights, w_gate=w_gate, w_up=w_up, w_down=w_down, final_gain=final_gain)


EPS = 1e-06

def slot_table(route_rows):
    flattened = route_rows.reshape(-1)
    matches = (flattened[:, None] == jnp.arange(EXPERTS, dtype=jnp.int32)[None, :]).astype(jnp.int32)
    earlier = jnp.cumsum(matches, axis=0) - matches
    slot_of = lax.optimization_barrier(jnp.sum(earlier * matches, axis=1))
    return (flattened * CAP + slot_of).reshape(route_rows.shape).astype(jnp.int32)

def dispatch(place_block, row_block):
    slot_ids = jnp.arange(EXPERTS * CAP, dtype=jnp.int32)
    selector = lax.optimization_barrier(jnp.sum((place_block[None, :, :] == slot_ids[:, None, None]).astype(jnp.float32), axis=2))
    return jnp.dot(selector.astype(jnp.bfloat16), row_block, preferred_element_type=jnp.float32).astype(jnp.bfloat16)

def expert(inputs):
    row_block, gate_w, up_w, down_w = inputs
    gate_value = jnp.dot(row_block, gate_w, preferred_element_type=jnp.float32)
    up_value = jnp.dot(row_block, up_w, preferred_element_type=jnp.float32)
    hidden = (jax.nn.silu(gate_value) * up_value).astype(jnp.bfloat16)
    hidden_split = hidden.reshape(row_block.shape[0], N_TP, FF // N_TP).astype(jnp.float32)
    down_split = down_w.reshape(N_TP, FF // N_TP, D).astype(jnp.float32)
    partial_value = jnp.einsum('rjf,jfd->jrd', hidden_split, down_split).astype(jnp.bfloat16)
    partial_value = lax.optimization_barrier(partial_value)
    return lax.optimization_barrier(jnp.sum(partial_value.astype(jnp.float32), axis=0)).astype(jnp.bfloat16)

def reference(tokens, norm_gain, routes, route_weights, w_gate, w_up, w_down, final_gain):
    tokens_f = tokens.astype(jnp.float32)
    inverse = lax.rsqrt(lax.optimization_barrier(jnp.mean(tokens_f * tokens_f, axis=1, keepdims=True)) + EPS)
    normed = (tokens_f * inverse * norm_gain[None, :]).astype(jnp.bfloat16)
    blocks = normed.reshape(N_EP, TOK_DEV, D)
    places = jax.vmap(slot_table)(routes.reshape(N_EP, TOK_DEV, TOP_K))
    buffers = jax.vmap(dispatch)(places, blocks)
    expert_in = buffers.reshape(N_EP, EXPERTS, CAP, D).transpose(1, 0, 2, 3).reshape(EXPERTS, N_EP * CAP, D)
    expert_out = lax.map(expert, (expert_in, w_gate, w_up, w_down))
    by_block = expert_out.reshape(EXPERTS, N_EP, CAP, D).transpose(1, 0, 2, 3).reshape(N_EP, EXPERTS * CAP, D)
    block_ids = jnp.arange(N_EP, dtype=jnp.int32)[:, None, None]
    picked = by_block[block_ids, places].astype(jnp.float32)
    weights = route_weights.reshape(N_EP, TOK_DEV, TOP_K)
    combined = lax.optimization_barrier(jnp.sum(weights[:, :, :, None] * picked, axis=2)).reshape(TOKENS, D)
    inverse_out = lax.rsqrt(lax.optimization_barrier(jnp.mean(combined * combined, axis=1, keepdims=True)) + EPS)
    return (combined * inverse_out * final_gain[None, :]).astype(jnp.bfloat16)
```

```python
import functools

import jax
import jax.numpy as jnp
from jax import lax
from jax.experimental import pallas as pl
from jax.experimental.pallas import tpu as pltpu
from jax.sharding import PartitionSpec as P

TOP_K = 6
EPS = 1e-06
MESH = pl.DeviceIdType.MESH
BF16, F32, I32 = jnp.bfloat16, jnp.float32, jnp.int32
CORES = 2


def wrap(value, count):
    return lax.rem(value + 4 * count, count)


def kernel(
    ep, tp, cap,
    tokens, norm_gain, routes, route_weights, w_gate, w_up, w_down, final_gain,
    out,
    tok, tab, rows, part, rs_long, rs_short, ret, results, squares,
    tok_in, gain_in, routes_in, weights_in, wgu, wd, final_in, c_hi, c_lo,
    in_sem, z_send, z_recv, d_send, d_recv, x_send, x_recv, l_send, l_recv, s_send, s_recv,
    r_send, r_recv, q_send, q_recv,
):
    e = lax.axis_index("ep")
    x = lax.axis_index("tp")
    z, c = lax.div(e, CORES), lax.rem(e, CORES)
    nz = ep // CORES
    steps = nz // 2
    zs = tp - 2
    back = tp // 2 - 2
    hl, hs = tp // 2, tp - 1 - tp // 2
    blk = tok_in.shape[1]
    share = tok_in.shape[2]
    last = steps - 1
    half = zs // 2

    def dev(zz, cc):
        return wrap(zz, nz) * CORES + cc

    up_z, down_z, partner = dev(z + 1, c), dev(z - 1, c), dev(z, 1 - c)
    x_right, x_left = wrap(x + 1, tp), wrap(x - 1, tp)
    dl = 1 - 2 * c
    x_long, x_short = wrap(x + dl, tp), wrap(x - dl, tp)

    barrier = pltpu.get_barrier_semaphore()
    for who in ({"ep": up_z}, {"ep": down_z}, {"ep": partner}, {"tp": x_right}, {"tp": x_left}):
        pl.semaphore_signal(barrier, inc=1, device_id=who, device_id_type=MESH)

    def lanes(q):
        return pl.ds(pl.multiple_of(wrap(x - back + q, tp) * share, share), share)

    first = []
    for q in range(tp):
        first.append(pltpu.make_async_copy(tokens.at[:, lanes(q)], tok_in.at[q], in_sem.at[0, q]))
        first.append(pltpu.make_async_copy(norm_gain.at[:, lanes(q)], gain_in.at[q], in_sem.at[1, q]))
    first.append(pltpu.make_async_copy(routes, routes_in, in_sem.at[2, 0]))
    first.append(pltpu.make_async_copy(route_weights, weights_in, in_sem.at[2, 1]))
    first.append(pltpu.make_async_copy(final_gain, final_in, in_sem.at[2, 2]))
    for copy in first:
        copy.start()
    later = []
    for q in range(tp):
        later.append(pltpu.make_async_copy(w_gate.at[0, lanes(q), :], wgu.at[q, :, 0:share], in_sem.at[3, q]))
        later.append(pltpu.make_async_copy(w_up.at[0, lanes(q), :], wgu.at[q, :, share:2 * share], in_sem.at[4, q]))
        owner = pl.ds(pl.multiple_of(wrap(x + q * dl, tp) * share, share), share)
        later.append(pltpu.make_async_copy(w_down.at[0, :, owner], wd.at[q], in_sem.at[5, q]))
    for copy in later:
        copy.start()
    for copy in first:
        copy.wait()

    total = jnp.zeros((blk, 1), F32)
    for q in range(tp):
        value = tok_in[q].astype(F32)
        total = total + jnp.sum(value * value, axis=1, keepdims=True)
    inverse = lax.rsqrt(total / (tp * share) + EPS)
    for q in range(zs):
        value = tok_in[q].astype(F32) * inverse * gain_in[q]
        tok[last, q, blk:2 * blk, :] = value.astype(BF16)

    expert_ids = lax.broadcasted_iota(I32, (blk, ep), 1)
    hits = jnp.zeros((blk, ep), F32)
    wt = jnp.zeros((blk, ep), F32)
    for k in range(TOP_K):
        hit = routes_in[:, k:k + 1] == expert_ids
        hits = hits + jnp.where(hit, 1.0, 0.0)
        wt = wt + jnp.where(hit, weights_in[:, k:k + 1], 0.0)
    hits_b = hits.astype(BF16)
    row_t = lax.broadcasted_iota(I32, (blk, 2 * blk), 0)
    lane_t = lax.broadcasted_iota(I32, (blk, 2 * blk), 1)
    lane_t = jnp.where(lane_t >= blk, lane_t - blk, lane_t)
    earlier = jnp.where(row_t < lane_t, 1.0, 0.0).astype(BF16)
    same = jnp.where(row_t == lane_t, 1.0, 0.0).astype(BF16)
    over = (((0,), (0,)), ((), ()))
    slot_t = lax.dot_general(hits_b, earlier, over, preferred_element_type=F32)
    hits_t = lax.dot_general(hits_b, same, over, preferred_element_type=F32)
    tab[last, 1] = (hits_t * (slot_t + 1.0)).astype(BF16)

    own = slice(blk, 2 * blk)
    plus, minus = slice(0, blk), slice(blk, 2 * blk)
    halves = (slice(0, half), slice(half, zs))

    def z_copy(dst_slot, way, piece, to, src_slot, src_tok, src_tab, dst_tok, dst_tab):
        if piece < 2:
            src, dst = tok.at[src_slot, halves[piece], src_tok, :], tok.at[dst_slot, halves[piece], dst_tok, :]
        else:
            src, dst = tab.at[src_slot, src_tab], tab.at[dst_slot, dst_tab]
        return pltpu.make_async_remote_copy(
            src, dst, z_send.at[dst_slot, way, piece], z_recv.at[dst_slot, way, piece],
            device_id={"ep": to}, device_id_type=MESH)

    def z_own(way, piece):
        return z_copy(0, way, piece, (up_z, down_z)[way], last, own, 1, (plus, minus)[way], way)

    def z_next(slot, way, piece):
        where = (plus, minus)[way]
        return z_copy(slot + 1, way, piece, (up_z, down_z)[way], slot, where, way, where, way)

    def z_end(piece):
        there = pl.ds(pl.multiple_of(c * blk, blk), blk)
        return z_copy(last, 0, piece, jnp.where(c == 0, up_z, down_z), last - 1, there, c, plus, 0)

    def z_done(slot, way, piece):
        where = (plus, minus)[way]
        ref = tok.at[slot, halves[piece], where, :] if piece < 2 else tab.at[slot, way]
        return pltpu.make_async_remote_copy(
            ref, ref, z_send.at[slot, way, piece], z_recv.at[slot, way, piece],
            device_id={"ep": up_z}, device_id_type=MESH)

    pl.semaphore_wait(barrier, 5)
    for piece in (2, 0, 1):
        for way in range(2):
            z_own(way, piece).start()

    t_row = lax.broadcasted_iota(I32, (blk, blk), 0)
    t_col = lax.broadcasted_iota(I32, (blk, blk), 1)
    before = jnp.where(t_col < t_row, 1.0, 0.0).astype(BF16)
    slot = jnp.dot(before, hits_b, preferred_element_type=F32)
    slot1 = (hits * (slot + 1.0)).astype(BF16)
    lane = lax.broadcasted_iota(I32, (ep, ep * cap), 1)
    start = lax.broadcasted_iota(I32, (ep, ep * cap), 0) * cap
    past = lane >= start
    inside = jnp.where(past & (lane < start + cap), 1.0, 0.0)
    spread = inside.astype(BF16)
    want = jnp.sum(inside * (lane - start + 1).astype(F32), axis=0, keepdims=True)
    wt_hi = wt.astype(BF16)
    wt_lo = (wt - wt_hi.astype(F32)).astype(BF16)
    match = jnp.dot(slot1, spread, preferred_element_type=F32) == want
    c_hi[...] = jnp.where(match, jnp.dot(wt_hi, spread, preferred_element_type=F32), 0.0).astype(BF16)
    c_lo[...] = jnp.where(match, jnp.dot(wt_lo, spread, preferred_element_type=F32), 0.0).astype(BF16)

    for copy in later:
        copy.wait()

    def d_copy(slot, piece):
        if piece < 2:
            src, dst = tok.at[slot, halves[piece], 0:2 * blk, :], tok.at[slot, halves[piece], 2 * blk:4 * blk, :]
        else:
            src, dst = tab.at[slot, 0:2], tab.at[slot, 2:4]
        return pltpu.make_async_remote_copy(
            src, dst, d_send.at[slot, piece], d_recv.at[slot, piece],
            device_id={"ep": partner}, device_id_type=MESH)

    def x_copy(slot, way):
        src, dst, to = ((zs - 1, tp - 2, x_left), (0, tp - 1, x_right))[way]
        return pltpu.make_async_remote_copy(
            rows.at[slot, src], rows.at[slot, dst], x_send.at[slot, way], x_recv.at[slot, way],
            device_id={"tp": to}, device_id_type=MESH)

    def long_copy(slot, hop):
        src = part.at[slot, hl] if hop == 1 else rs_long.at[slot, hop - 2]
        return pltpu.make_async_remote_copy(
            src, rs_long.at[slot, hop - 1], l_send.at[slot, hop - 1], l_recv.at[slot, hop - 1],
            device_id={"tp": x_long}, device_id_type=MESH)

    def short_copy(slot, hop):
        src = part.at[slot, tp - hs] if hop == 1 else rs_short.at[slot, hop - 2]
        return pltpu.make_async_remote_copy(
            src, rs_short.at[slot, hop - 1], s_send.at[slot, hop - 1], s_recv.at[slot, hop - 1],
            device_id={"tp": x_short}, device_id_type=MESH)

    def ret_copy(slot, j, to):
        return pltpu.make_async_remote_copy(
            ret.at[slot, j], results.at[e], r_send.at[slot, j], r_recv.at[0],
            device_id={"ep": to}, device_id_type=MESH)

    def arrive(slot, piece):
        @pl.when(slot < last)
        def _():
            z_done(slot, 0, piece).wait_recv()
            z_done(slot, 1, piece).wait_recv()

            @pl.when(slot < last - 1)
            def _():
                z_next(slot, 0, piece).start()
                z_next(slot, 1, piece).start()

            @pl.when(slot == last - 1)
            def _():
                z_end(piece).start()

        @pl.when(slot == last)
        def _():
            z_done(slot, 0, piece).wait_recv()

        @pl.when(slot <= last)
        def _():
            d_copy(slot, piece).start()

    rows_all = 4 * cap
    r_id = lax.broadcasted_iota(I32, (rows_all, 4 * blk), 0)
    l_id = lax.broadcasted_iota(I32, (rows_all, 4 * blk), 1)
    my_slot = jnp.full((rows_all, 4 * blk), -1.0, F32)
    for j in range(4):
        good = (r_id >= j * cap) & (r_id < (j + 1) * cap) & (l_id >= j * blk) & (l_id < (j + 1) * blk)
        my_slot = jnp.where(good, (r_id - j * cap + 1).astype(F32), my_slot)
    left_half = lax.broadcasted_iota(I32, (1, 2 * blk), 1) < blk
    my_expert = lax.broadcasted_iota(I32, (ep, 2 * blk), 0) == e

    def pick(slot):
        for piece in range(3):
            d_copy(slot, piece).wait_recv()
        seen = []
        for j in range(4):
            seen.append(jnp.sum(jnp.where(my_expert, tab[slot, j].astype(F32), 0.0), axis=0, keepdims=True))
        pair = jnp.concatenate(
            [jnp.where(left_half, seen[0], seen[1]), jnp.where(left_half, seen[2], seen[3])], axis=1)
        choose = jnp.where(my_slot == pair, 1.0, 0.0).astype(BF16)

        def one(q):
            rows[slot, q] = jnp.dot(choose, tok[slot, q], preferred_element_type=F32).astype(BF16)

        one(zs - 1)
        x_copy(slot, 0).start()
        one(0)
        x_copy(slot, 1).start()
        for q in range(1, zs - 1):
            one(q)

    def compute(slot):
        acc = jnp.zeros((rows_all, 2 * share), F32)
        for q in range(zs):
            acc = acc + jnp.dot(rows[slot, q], wgu[q], preferred_element_type=F32)
        x_copy(slot, 0).wait_recv()
        x_copy(slot, 1).wait_recv()
        for q in range(zs, tp):
            acc = acc + jnp.dot(rows[slot, q], wgu[q], preferred_element_type=F32)
        gate, up = acc[:, :share], acc[:, share:]
        hidden = (gate / (1.0 + jnp.exp(-gate)) * up).astype(BF16)

        def one(q):
            part[slot, q] = jnp.dot(hidden, wd[q], preferred_element_type=F32).astype(BF16)

        one(hl)
        long_copy(slot, 1).start()
        one(tp - hs)
        short_copy(slot, 1).start()
        for q in range(tp):
            if q not in (hl, tp - hs):
                one(q)

    def hop(slot, h):
        long_copy(slot, h).wait_recv()
        rs_long[slot, h - 1] = (rs_long[slot, h - 1].astype(F32) + part[slot, hl - h].astype(F32)).astype(BF16)
        long_copy(slot, h + 1).start()
        if h < hs:
            short_copy(slot, h).wait_recv()
            rs_short[slot, h - 1] = (
                rs_short[slot, h - 1].astype(F32) + part[slot, tp - hs + h].astype(F32)).astype(BF16)
            short_copy(slot, h + 1).start()

    def finish(slot):
        long_copy(slot, hl).wait_recv()
        short_copy(slot, hs).wait_recv()
        value = part[slot, 0].astype(F32) + rs_long[slot, hl - 1].astype(F32) + rs_short[slot, hs - 1].astype(F32)
        for j in range(4):
            ret[slot, j] = value[j * cap:(j + 1) * cap].astype(BF16)

        @pl.when(slot < last)
        def _():
            for j in range(4):
                ret_copy(slot, j, dev(z + (-1, 1)[j % 2] * (slot + 1), (c, 1 - c)[j // 2])).start()

        @pl.when(slot == last)
        def _():
            ret_copy(slot, 0, dev(z + steps, c)).start()
            ret_copy(slot, 2, dev(z + steps, 1 - c)).start()
            ret_copy(slot, 3, partner).start()
            results[e] = ret[slot, 1]

    def at(turn, behind, act):
        @pl.when((turn >= behind) & (turn - behind <= last))
        def _():
            act(turn - behind)

    def turn(t, carry):
        arrive(t, 2)
        arrive(t, 0)
        at(t, hl + 1, finish)
        for h in range(hl - 1, 0, -1):
            at(t, h + 1, lambda s, h=h: hop(s, h))
        at(t, 1, compute)
        arrive(t, 1)
        at(t, 0, pick)
        return carry

    lax.fori_loop(0, steps + hl + 1, turn, 0)

    pltpu.make_async_copy(results.at[0:ep - 1], results.at[0:ep - 1], r_recv.at[0]).wait()
    got = results[...].astype(F32).reshape(ep * cap, share).astype(BF16)
    combined = jnp.dot(c_hi[...], got, preferred_element_type=F32) + jnp.dot(
        c_lo[...], got, preferred_element_type=F32)
    own_sq = jnp.sum(combined * combined, axis=1, keepdims=True)
    eye = t_row == t_col
    flat = jnp.sum(jnp.where(eye, jnp.broadcast_to(own_sq, (blk, blk)), 0.0), axis=0, keepdims=True)
    squares[x] = jnp.broadcast_to(jnp.concatenate([flat, flat], axis=1), squares.shape[1:])

    def q_copy(q):
        return pltpu.make_async_remote_copy(
            squares.at[x], squares.at[x], q_send.at[q], q_recv.at[0],
            device_id={"tp": wrap(x + q, tp)}, device_id_type=MESH)

    for q in range(1, tp):
        q_copy(q).start()

    def drain(slot, carry):
        for piece in range(3):
            d_copy(slot, piece).wait_send()

            @pl.when(slot < last)
            def _(piece=piece):
                z_done(slot, 0, piece).wait_send()
                z_done(slot, 1, piece).wait_send()

            @pl.when(slot == last)
            def _(piece=piece):
                z_done(slot, 0, piece).wait_send()
        for way in range(2):
            x_copy(slot, way).wait_send()
        for h in range(1, hl + 1):
            long_copy(slot, h).wait_send()
        for h in range(1, hs + 1):
            short_copy(slot, h).wait_send()
        for j in (0, 2, 3):
            ret_copy(slot, j, partner).wait_send()

        @pl.when(slot < last)
        def _():
            ret_copy(slot, 1, partner).wait_send()

        return carry

    lax.fori_loop(0, steps, drain, 0)
    for q in range(1, tp):
        q_copy(q).wait_send()
    pltpu.make_async_copy(squares.at[0:tp - 1], squares.at[0:tp - 1], q_recv.at[0]).wait()
    everyone = jnp.sum(squares[...], axis=0)[0:1, 0:blk]
    column = jnp.sum(jnp.where(eye, jnp.broadcast_to(everyone, (blk, blk)), 0.0), axis=1, keepdims=True)
    scale = lax.rsqrt(column / (tp * share) + EPS)
    out[...] = (combined * scale * final_in[...]).astype(out.dtype)


def solution(mesh):
    ep, tp = mesh.shape["ep"], mesh.shape["tp"]

    def per_device(tokens, norm_gain, routes, route_weights, w_gate, w_up, w_down, final_gain):
        blk, features = tokens.shape
        cap = max(2, min(blk, 2 * blk * TOP_K // ep))
        share = features // tp
        steps = ep // CORES // 2
        hl, hs = tp // 2, tp - 1 - tp // 2
        zs = tp - 2
        dma = pltpu.SemaphoreType.DMA
        vmem = pltpu.VMEM
        return pl.pallas_call(
            functools.partial(kernel, ep, tp, cap),
            out_shape=jax.ShapeDtypeStruct((blk, share), BF16),
            in_specs=[pl.BlockSpec(memory_space=pl.ANY)] * 8,
            out_specs=pl.BlockSpec(memory_space=pltpu.VMEM),
            scratch_shapes=[
                vmem((steps, zs, 4 * blk, share), BF16),
                vmem((steps, 4, ep, 2 * blk), BF16),
                vmem((steps, tp, 4 * cap, share), BF16),
                vmem((steps, tp, 4 * cap, share), BF16),
                vmem((steps, hl, 4 * cap, share), BF16),
                vmem((steps, hs, 4 * cap, share), BF16),
                vmem((steps, 4, cap, share), BF16),
                vmem((ep, cap, share), BF16),
                vmem((tp, 8, 2 * blk), F32),
                vmem((tp, blk, share), BF16),
                vmem((tp, 1, share), F32),
                vmem((blk, TOP_K), I32),
                vmem((blk, TOP_K), F32),
                vmem((tp, share, 2 * share), BF16),
                vmem((tp, share, share), BF16),
                vmem((1, share), F32),
                vmem((blk, ep * cap), BF16),
                vmem((blk, ep * cap), BF16),
                dma((6, tp)),
                dma((steps, 2, 3)), dma((steps, 2, 3)),
                dma((steps, 3)), dma((steps, 3)),
                dma((steps, 2)), dma((steps, 2)),
                dma((steps, hl)), dma((steps, hl)),
                dma((steps, hs)), dma((steps, hs)),
                dma((steps, 4)), dma((1,)),
                dma((tp,)), dma((1,)),
            ],
            compiler_params=pltpu.CompilerParams(
                collective_id=0, has_side_effects=True, vmem_limit_bytes=56 * 1024 * 1024),
        )(tokens, norm_gain.reshape(1, features), routes, route_weights, w_gate, w_up, w_down,
          final_gain.reshape(1, share))

    placed = (
        P(("grp", "ep"), None),
        P(),
        P(("grp", "ep"), None),
        P(("grp", "ep"), None),
        P("ep", None, "tp"),
        P("ep", None, "tp"),
        P("ep", "tp", None),
        P("tp"),
    )
    return jax.shard_map(
        per_device, mesh=mesh, in_specs=placed, out_specs=P(("grp", "ep"), "tp"), check_vma=False
    )
```

```python
import functools

import jax
import jax.numpy as jnp
from jax import lax
from jax.experimental import pallas as pl
from jax.experimental.pallas import tpu as pltpu
from jax.sharding import PartitionSpec as P

TOP_K = 6
EPS = 1e-06
MESH = pl.DeviceIdType.MESH
BF16, F32, I32 = jnp.bfloat16, jnp.float32, jnp.int32
CORES = 2


def wrap(value, count):
    return lax.rem(value + 4 * count, count)


def kernel(
    ep, tp, cap,
    tokens, norm_gain, routes, route_weights, w_gate, w_up, w_down, final_gain,
    out,
    tok, tab, rows, part, rs_long, rs_short, ret, results, squares,
    tok_in, gain_in, routes_in, weights_in, wgu, wd, final_in, c_hi, c_lo,
    in_sem, z_send, z_recv, d_send, d_recv, x_send, x_recv, l_send, l_recv, s_send, s_recv,
    r_send, r_recv, q_send, q_recv,
):
    e = lax.axis_index("ep")
    x = lax.axis_index("tp")
    z, c = lax.div(e, CORES), lax.rem(e, CORES)
    nz = ep // CORES
    steps = nz // 2
    zs = tp - 2
    back = tp // 2 - 2
    hl, hs = tp // 2, tp - 1 - tp // 2
    blk = tok_in.shape[1]
    share = tok_in.shape[2]
    last, mine = steps - 1, steps
    half = zs // 2

    def dev(zz, cc):
        return wrap(zz, nz) * CORES + cc

    up_z, down_z, partner = dev(z + 1, c), dev(z - 1, c), dev(z, 1 - c)
    x_right, x_left = wrap(x + 1, tp), wrap(x - 1, tp)
    dl = 1 - 2 * c
    x_long, x_short = wrap(x + dl, tp), wrap(x - dl, tp)

    barrier = pltpu.get_barrier_semaphore()
    for who in ({"ep": up_z}, {"ep": down_z}, {"ep": partner}, {"tp": x_right}, {"tp": x_left}):
        pl.semaphore_signal(barrier, inc=1, device_id=who, device_id_type=MESH)

    def lanes(q):
        return pl.ds(pl.multiple_of(wrap(x - back + q, tp) * share, share), share)

    first, second, later = [], [], []
    for q in range(tp):
        first.append(pltpu.make_async_copy(tokens.at[:, lanes(q)], tok_in.at[q], in_sem.at[0, q]))
        first.append(pltpu.make_async_copy(norm_gain.at[:, lanes(q)], gain_in.at[q], in_sem.at[1, q]))
    second.append(pltpu.make_async_copy(routes, routes_in, in_sem.at[2, 0]))
    second.append(pltpu.make_async_copy(route_weights, weights_in, in_sem.at[2, 1]))
    second.append(pltpu.make_async_copy(final_gain, final_in, in_sem.at[2, 2]))
    for q in range(tp):
        rows_q = slice(q * share, (q + 1) * share)
        later.append(pltpu.make_async_copy(w_gate.at[0, lanes(q), :], wgu.at[rows_q, 0:share], in_sem.at[3, q]))
        later.append(pltpu.make_async_copy(w_up.at[0, lanes(q), :], wgu.at[rows_q, share:2 * share], in_sem.at[4, q]))
        owner = pl.ds(pl.multiple_of(wrap(x + q * dl, tp) * share, share), share)
        later.append(pltpu.make_async_copy(w_down.at[0, :, owner], wd.at[q], in_sem.at[5, q]))
    for copy in first + second + later:
        copy.start()

    near, far = slice(0, blk), slice(blk, 2 * blk)
    halves = (slice(0, half), slice(half, zs))

    def z_copy(dst_slot, way, piece, to, src_slot, src_tok, src_tab, dst_tok, dst_tab):
        if piece < 2:
            src, dst = tok.at[src_slot, halves[piece], src_tok, :], tok.at[dst_slot, halves[piece], dst_tok, :]
        else:
            src, dst = tab.at[src_slot, src_tab], tab.at[dst_slot, dst_tab]
        return pltpu.make_async_remote_copy(
            src, dst, z_send.at[dst_slot, way, piece], z_recv.at[dst_slot, way, piece],
            device_id={"ep": to}, device_id_type=MESH)

    def z_own(way, piece):
        return z_copy(0, way, piece, (up_z, down_z)[way], mine, near, 0, (near, far)[way], way)

    def z_next(slot, way, piece):
        where = (near, far)[way]
        return z_copy(slot + 1, way, piece, (up_z, down_z)[way], slot, where, way, where, way)

    def z_end(piece):
        there = pl.ds(pl.multiple_of(c * blk, blk), blk)
        return z_copy(last, 0, piece, jnp.where(c == 0, up_z, down_z), last - 1, there, c, near, 0)

    def z_done(slot, way, piece):
        where = (near, far)[way]
        ref = tok.at[slot, halves[piece], where, :] if piece < 2 else tab.at[slot, way]
        return pltpu.make_async_remote_copy(
            ref, ref, z_send.at[slot, way, piece], z_recv.at[slot, way, piece],
            device_id={"ep": up_z}, device_id_type=MESH)

    def d_copy(slot, piece, n):
        h = n // 2
        if piece < 2:
            src = tok.at[slot, halves[piece], 0:h * blk, :]
            dst = tok.at[slot, halves[piece], h * blk:n * blk, :]
        else:
            src, dst = tab.at[slot, 0:h], tab.at[slot, h:n]
        return pltpu.make_async_remote_copy(
            src, dst, d_send.at[slot, piece], d_recv.at[slot, piece],
            device_id={"ep": partner}, device_id_type=MESH)

    def x_copy(slot, way, n):
        src, dst, to = ((zs - 1, tp - 2, x_left), (0, tp - 1, x_right))[way]
        return pltpu.make_async_remote_copy(
            rows.at[slot, 0:n * cap, src * share:(src + 1) * share],
            rows.at[slot, 0:n * cap, dst * share:(dst + 1) * share],
            x_send.at[slot, way], x_recv.at[slot, way], device_id={"tp": to}, device_id_type=MESH)

    def long_copy(slot, hop, n):
        top = slice(0, n * cap)
        src = part.at[slot, hl, top] if hop == 1 else rs_long.at[slot, hop - 2, top]
        return pltpu.make_async_remote_copy(
            src, rs_long.at[slot, hop - 1, top], l_send.at[slot, hop - 1], l_recv.at[slot, hop - 1],
            device_id={"tp": x_long}, device_id_type=MESH)

    def short_copy(slot, hop, n):
        top = slice(0, n * cap)
        src = part.at[slot, tp - hs, top] if hop == 1 else rs_short.at[slot, hop - 2, top]
        return pltpu.make_async_remote_copy(
            src, rs_short.at[slot, hop - 1, top], s_send.at[slot, hop - 1], s_recv.at[slot, hop - 1],
            device_id={"tp": x_short}, device_id_type=MESH)

    def ret_copy(slot, j, to):
        return pltpu.make_async_remote_copy(
            ret.at[slot, j], results.at[e], r_send.at[slot, j], r_recv.at[0],
            device_id={"ep": to}, device_id_type=MESH)

    for copy in first:
        copy.wait()
    total = jnp.zeros((blk, 1), F32)
    for q in range(tp):
        value = tok_in[q].astype(F32)
        total = total + jnp.sum(value * value, axis=1, keepdims=True)
    inverse = lax.rsqrt(total / (tp * share) + EPS)

    def norm(q):
        value = tok_in[q].astype(F32) * inverse * gain_in[q]
        tok[mine, q, near, :] = value.astype(BF16)

    for q in range(half):
        norm(q)
    pl.semaphore_wait(barrier, 5)
    z_own(0, 0).start()
    z_own(1, 0).start()
    for q in range(half, zs):
        norm(q)
    z_own(0, 1).start()
    z_own(1, 1).start()
    d_copy(mine, 0, 2).start()
    d_copy(mine, 1, 2).start()

    for copy in second:
        copy.wait()
    expert_ids = lax.broadcasted_iota(I32, (ep, blk), 0)
    hits = jnp.zeros((ep, blk), F32)
    wt = jnp.zeros((ep, blk), F32)
    for k in range(TOP_K):
        hit = routes_in[k:k + 1, :] == expert_ids
        hits = hits + jnp.where(hit, 1.0, 0.0)
        wt = wt + jnp.where(hit, weights_in[k:k + 1, :], 0.0)
    hits_b = hits.astype(BF16)
    row_t = lax.broadcasted_iota(I32, (blk, 2 * blk), 0)
    lane_t = lax.broadcasted_iota(I32, (blk, 2 * blk), 1)
    lane_t = jnp.where(lane_t >= blk, lane_t - blk, lane_t)
    earlier = jnp.where(row_t < lane_t, 1.0, 0.0).astype(BF16)
    same = jnp.where(row_t == lane_t, 1.0, 0.0).astype(BF16)
    slots = jnp.dot(hits_b, same, preferred_element_type=F32) * (
        jnp.dot(hits_b, earlier, preferred_element_type=F32) + 1.0)
    tab[mine, 0] = slots.astype(BF16)
    z_own(0, 2).start()
    z_own(1, 2).start()
    d_copy(mine, 2, 2).start()

    over = (((0,), (0,)), ((), ()))
    slot1 = slots[:, 0:blk].astype(BF16)
    lane = lax.broadcasted_iota(I32, (ep, ep * cap), 1)
    start = lax.broadcasted_iota(I32, (ep, ep * cap), 0) * cap
    inside = jnp.where((lane >= start) & (lane < start + cap), 1.0, 0.0)
    spread = inside.astype(BF16)
    want = jnp.sum(inside * (lane - start + 1).astype(F32), axis=0, keepdims=True)
    wt_hi = wt.astype(BF16)
    wt_lo = (wt - wt_hi.astype(F32)).astype(BF16)
    match = lax.dot_general(slot1, spread, over, preferred_element_type=F32) == want
    c_hi[...] = jnp.where(
        match, lax.dot_general(wt_hi, spread, over, preferred_element_type=F32), 0.0).astype(BF16)
    c_lo[...] = jnp.where(
        match, lax.dot_general(wt_lo, spread, over, preferred_element_type=F32), 0.0).astype(BF16)

    for copy in later:
        copy.wait()

    def arrive(slot, piece):
        @pl.when(slot < last)
        def _():
            z_done(slot, 0, piece).wait_recv()
            z_done(slot, 1, piece).wait_recv()

            @pl.when(slot < last - 1)
            def _():
                z_next(slot, 0, piece).start()
                z_next(slot, 1, piece).start()

            @pl.when(slot == last - 1)
            def _():
                z_end(piece).start()

            d_copy(slot, piece, 4).start()

        @pl.when(slot == last)
        def _():
            z_done(slot, 0, piece).wait_recv()
            d_copy(slot, piece, 2).start()

    left_half = lax.broadcasted_iota(I32, (1, 2 * blk), 1) < blk
    my_expert = lax.broadcasted_iota(I32, (ep, 2 * blk), 0) == e

    def pick(slot, n):
        r_id = lax.broadcasted_iota(I32, (n * cap, n * blk), 0)
        l_id = lax.broadcasted_iota(I32, (n * cap, n * blk), 1)
        my_slot = jnp.full((n * cap, n * blk), -1, I32)
        for j in range(n):
            good = (r_id >= j * cap) & (r_id < (j + 1) * cap) & (l_id >= j * blk) & (l_id < (j + 1) * blk)
            my_slot = jnp.where(good, r_id - j * cap + 1, my_slot)
        for piece in range(3):
            d_copy(slot, piece, n).wait_recv()
        seen = []
        for j in range(n):
            seen.append(jnp.sum(jnp.where(my_expert, tab[slot, j].astype(F32), 0.0), axis=0, keepdims=True))
        pair = jnp.concatenate(
            [jnp.where(left_half, seen[j], seen[j + 1]) for j in range(0, n, 2)], axis=1)
        choose = jnp.where(my_slot.astype(F32) == pair, 1.0, 0.0).astype(BF16)

        def one(q):
            rows[slot, 0:n * cap, q * share:(q + 1) * share] = jnp.dot(
                choose, tok[slot, q, 0:n * blk, :], preferred_element_type=F32).astype(BF16)

        one(zs - 1)
        x_copy(slot, 0, n).start()
        one(0)
        x_copy(slot, 1, n).start()
        for q in range(1, zs - 1):
            one(q)

    def compute(slot, n):
        x_copy(slot, 0, n).wait_recv()
        x_copy(slot, 1, n).wait_recv()
        acc = jnp.dot(rows[slot, 0:n * cap, :], wgu[...], preferred_element_type=F32)
        gate, up = acc[:, :share], acc[:, share:]
        hidden = (gate / (1.0 + jnp.exp(-gate)) * up).astype(BF16)

        def one(q):
            part[slot, q, 0:n * cap] = jnp.dot(hidden, wd[q], preferred_element_type=F32).astype(BF16)

        one(hl)
        long_copy(slot, 1, n).start()
        one(tp - hs)
        short_copy(slot, 1, n).start()
        for q in range(tp):
            if q not in (hl, tp - hs):
                one(q)

    def hop(slot, n, h):
        top = slice(0, n * cap)
        long_copy(slot, h, n).wait_recv()
        rs_long[slot, h - 1, top] = (
            rs_long[slot, h - 1, top].astype(F32) + part[slot, hl - h, top].astype(F32)).astype(BF16)
        long_copy(slot, h + 1, n).start()
        if h < hs:
            short_copy(slot, h, n).wait_recv()
            rs_short[slot, h - 1, top] = (
                rs_short[slot, h - 1, top].astype(F32) + part[slot, tp - hs + h, top].astype(F32)).astype(BF16)
            short_copy(slot, h + 1, n).start()

    def finish(slot, n):
        top = slice(0, n * cap)
        long_copy(slot, hl, n).wait_recv()
        short_copy(slot, hs, n).wait_recv()
        value = (part[slot, 0, top].astype(F32) + rs_long[slot, hl - 1, top].astype(F32)
                 + rs_short[slot, hs - 1, top].astype(F32))
        for j in range(n):
            ret[slot, j] = value[j * cap:(j + 1) * cap].astype(BF16)
        if n == 4:
            for j in range(4):
                ret_copy(slot, j, dev(z + (-1, 1)[j % 2] * (slot + 1), (c, 1 - c)[j // 2])).start()
        else:
            @pl.when(slot == last)
            def _():
                ret_copy(slot, 0, dev(z + steps, c)).start()
                ret_copy(slot, 1, dev(z + steps, 1 - c)).start()

            @pl.when(slot == mine)
            def _():
                ret_copy(slot, 1, partner).start()
                results[e] = ret[slot, 0]

    def at(turn, behind, act):
        slot = turn - behind

        @pl.when((slot >= 0) & (slot < last))
        def _():
            act(slot, 4)

        @pl.when((slot == -1) | (slot == last))
        def _():
            act(jnp.where(slot < 0, mine, slot), 2)

    def turn(t, carry):
        arrive(t, 0)
        at(t, hl + 2, finish)
        for h in range(hl - 1, 0, -1):
            at(t, h + 2, functools.partial(hop, h=h))
        at(t, 1, pick)
        arrive(t, 1)
        arrive(t, 2)
        at(t, 2, compute)
        return carry

    lax.fori_loop(0, steps + hl + 2, turn, 0)

    pltpu.make_async_copy(results.at[0:ep - 1], results.at[0:ep - 1], r_recv.at[0]).wait()
    got = results[...].astype(F32).reshape(ep * cap, share).astype(BF16)
    combined = jnp.dot(c_hi[...], got, preferred_element_type=F32) + jnp.dot(
        c_lo[...], got, preferred_element_type=F32)
    own_sq = jnp.sum(combined * combined, axis=1, keepdims=True)
    eye = lax.broadcasted_iota(I32, (blk, blk), 0) == lax.broadcasted_iota(I32, (blk, blk), 1)
    flat = jnp.sum(jnp.where(eye, jnp.broadcast_to(own_sq, (blk, blk)), 0.0), axis=0, keepdims=True)
    squares[x] = jnp.broadcast_to(jnp.concatenate([flat, flat], axis=1), squares.shape[1:])

    def q_copy(q):
        return pltpu.make_async_remote_copy(
            squares.at[x], squares.at[x], q_send.at[q], q_recv.at[0],
            device_id={"tp": wrap(x + q, tp)}, device_id_type=MESH)

    for q in range(1, tp):
        q_copy(q).start()

    def left(slot, n):
        for piece in range(3):
            d_copy(slot, piece, n).wait_send()
        for way in range(2):
            x_copy(slot, way, n).wait_send()
        for h in range(1, hl + 1):
            long_copy(slot, h, n).wait_send()
        for h in range(1, hs + 1):
            short_copy(slot, h, n).wait_send()
        for j in range(1, n):
            ret_copy(slot, j, partner).wait_send()

    def drain(slot, carry):
        left(slot, 4)
        ret_copy(slot, 0, partner).wait_send()
        for piece in range(3):
            z_done(slot, 0, piece).wait_send()
            z_done(slot, 1, piece).wait_send()
        return carry

    lax.fori_loop(0, last, drain, 0)
    left(last, 2)
    left(mine, 2)
    ret_copy(last, 0, partner).wait_send()
    for piece in range(3):
        z_done(last, 0, piece).wait_send()
    for q in range(1, tp):
        q_copy(q).wait_send()
    pltpu.make_async_copy(squares.at[0:tp - 1], squares.at[0:tp - 1], q_recv.at[0]).wait()
    everyone = jnp.sum(squares[...], axis=0)[0:1, 0:blk]
    column = jnp.sum(jnp.where(eye, jnp.broadcast_to(everyone, (blk, blk)), 0.0), axis=1, keepdims=True)
    scale = lax.rsqrt(column / (tp * share) + EPS)
    out[...] = (combined * scale * final_in[...]).astype(out.dtype)


def solution(mesh):
    ep, tp = mesh.shape["ep"], mesh.shape["tp"]

    def per_device(tokens, norm_gain, routes, route_weights, w_gate, w_up, w_down, final_gain):
        blk, features = tokens.shape
        cap = max(2, min(blk, 2 * blk * TOP_K // ep))
        share = features // tp
        slots = ep // CORES // 2 + 1
        hl, hs = tp // 2, tp - 1 - tp // 2
        zs = tp - 2
        dma = pltpu.SemaphoreType.DMA
        vmem = pltpu.VMEM
        return pl.pallas_call(
            functools.partial(kernel, ep, tp, cap),
            out_shape=jax.ShapeDtypeStruct((blk, share), BF16),
            in_specs=[pl.BlockSpec(memory_space=pl.ANY)] * 8,
            out_specs=pl.BlockSpec(memory_space=pltpu.VMEM),
            scratch_shapes=[
                vmem((slots, zs, 4 * blk, share), BF16),
                vmem((slots, 4, ep, 2 * blk), BF16),
                vmem((slots, 4 * cap, features), BF16),
                vmem((slots, tp, 4 * cap, share), BF16),
                vmem((slots, hl, 4 * cap, share), BF16),
                vmem((slots, hs, 4 * cap, share), BF16),
                vmem((slots, 4, cap, share), BF16),
                vmem((ep, cap, share), BF16),
                vmem((tp, 8, 2 * blk), F32),
                vmem((tp, blk, share), BF16),
                vmem((tp, 1, share), F32),
                vmem((TOP_K, blk), I32),
                vmem((TOP_K, blk), F32),
                vmem((features, 2 * share), BF16),
                vmem((tp, share, share), BF16),
                vmem((1, share), F32),
                vmem((blk, ep * cap), BF16),
                vmem((blk, ep * cap), BF16),
                dma((6, tp)),
                dma((slots, 2, 3)), dma((slots, 2, 3)),
                dma((slots, 3)), dma((slots, 3)),
                dma((slots, 2)), dma((slots, 2)),
                dma((slots, hl)), dma((slots, hl)),
                dma((slots, hs)), dma((slots, hs)),
                dma((slots, 4)), dma((1,)),
                dma((tp,)), dma((1,)),
            ],
            compiler_params=pltpu.CompilerParams(
                collective_id=0, has_side_effects=True, vmem_limit_bytes=56 * 1024 * 1024),
        )(tokens, norm_gain.reshape(1, features), routes.T, route_weights.T, w_gate, w_up, w_down,
          final_gain.reshape(1, share))

    placed = (
        P(("grp", "ep"), None),
        P(),
        P(("grp", "ep"), None),
        P(("grp", "ep"), None),
        P("ep", None, "tp"),
        P("ep", None, "tp"),
        P("ep", "tp", None),
        P("tp"),
    )
    return jax.shard_map(
        per_device, mesh=mesh, in_specs=placed, out_specs=P(("grp", "ep"), "tp"), check_vma=False
    )
```

```python
import functools

import jax
import jax.numpy as jnp
from jax import lax
from jax.experimental import pallas as pl
from jax.experimental.pallas import tpu as pltpu
from jax.sharding import PartitionSpec as P

TOP_K = 6
EPS = 1e-06
MESH = pl.DeviceIdType.MESH
BF16, F32, I32 = jnp.bfloat16, jnp.float32, jnp.int32
CORES = 2
XS = 2


def wrap(value, count):
    return lax.rem(value + 4 * count, count)


def kernel(
    ep, tp, cap,
    tokens, norm_gain, routes, route_weights, w_gate, w_up, w_down, final_gain,
    out,
    tok, tab, rows, part, rs, direct, ret, results, squares,
    tok_in, gain_in, routes_in, weights_in, wgu, wd, final_in, c_hi, c_lo,
    in_sem, out_sem, z_recv, d_recv, x_recv, l_recv, t_recv, r_recv, q_recv,
):
    e = lax.axis_index("ep")
    x = lax.axis_index("tp")
    z, c = lax.div(e, CORES), lax.rem(e, CORES)
    nz = ep // CORES
    steps = nz // 2
    zs = tp - XS
    back = (zs - 1) // 2
    hl, hs = tp // 2, tp - 1 - tp // 2
    blk = tok_in.shape[1]
    share = tok_in.shape[2]
    last, mine = steps - 1, steps
    half = zs // 2

    def dev(zz, cc):
        return wrap(zz, nz) * CORES + cc

    up_z, down_z, partner = dev(z + 1, c), dev(z - 1, c), dev(z, 1 - c)
    x_right, x_left = wrap(x + 1, tp), wrap(x - 1, tp)
    dl = 1 - 2 * c
    x_long, x_short = wrap(x + dl, tp), wrap(x - dl, tp)

    barrier = pltpu.get_barrier_semaphore()
    for who in ({"ep": up_z}, {"ep": down_z}, {"ep": partner}, {"tp": x_right}, {"tp": x_left}):
        pl.semaphore_signal(barrier, inc=1, device_id=who, device_id_type=MESH)

    def lanes(q):
        return pl.ds(pl.multiple_of(wrap(x - back + q, tp) * share, share), share)

    for q in range(tp):
        pltpu.make_async_copy(tokens.at[:, lanes(q)], tok_in.at[q], in_sem.at[0]).start()
        pltpu.make_async_copy(norm_gain.at[:, lanes(q)], gain_in.at[q], in_sem.at[1]).start()
    second = [pltpu.make_async_copy(routes, routes_in, in_sem.at[2]),
              pltpu.make_async_copy(route_weights, weights_in, in_sem.at[3]),
              pltpu.make_async_copy(final_gain, final_in, in_sem.at[4])]
    for copy in second:
        copy.start()
    for q in range(tp):
        rows_q = slice(q * share, (q + 1) * share)
        pltpu.make_async_copy(w_gate.at[0, lanes(q), :], wgu.at[rows_q, 0:share], in_sem.at[5]).start()
        pltpu.make_async_copy(w_up.at[0, lanes(q), :], wgu.at[rows_q, share:2 * share], in_sem.at[5]).start()
        owner = pl.ds(pl.multiple_of(wrap(x + q * dl, tp) * share, share), share)
        pltpu.make_async_copy(w_down.at[0, :, owner], wd.at[q], in_sem.at[6]).start()

    def whole(ref, sem):
        return pltpu.make_async_copy(ref, ref, sem)

    near, far = slice(0, blk), slice(blk, 2 * blk)
    halves = (slice(0, half), slice(half, zs))

    def z_copy(dst_slot, piece, to, src_slot, src_tok, src_tab, dst_tok, dst_tab):
        if piece < 2:
            src, dst = tok.at[src_slot, halves[piece], src_tok, :], tok.at[dst_slot, halves[piece], dst_tok, :]
        else:
            src, dst = tab.at[src_slot, src_tab], tab.at[dst_slot, dst_tab]
        return pltpu.make_async_remote_copy(
            src, dst, out_sem.at[piece // 2], z_recv.at[dst_slot, piece],
            device_id={"ep": to}, device_id_type=MESH)

    def z_own(way, piece):
        return z_copy(0, piece, (up_z, down_z)[way], mine, near, 0, (near, far)[way], way)

    def z_next(slot, way, piece):
        where = (near, far)[way]
        return z_copy(slot + 1, piece, (up_z, down_z)[way], slot, where, way, where, way)

    def z_end(piece):
        there = pl.ds(pl.multiple_of(c * blk, blk), blk)
        return z_copy(last, piece, jnp.where(c == 0, up_z, down_z), last - 1, there, c, near, 0)

    def z_done(slot, piece, n):
        ref = tok.at[slot, halves[piece], 0:n * blk, :] if piece < 2 else tab.at[slot, 0:n]
        return whole(ref, z_recv.at[slot, piece])

    def d_copy(slot, piece, n):
        h = n // 2
        if piece < 2:
            src = tok.at[slot, halves[piece], 0:h * blk, :]
            dst = tok.at[slot, halves[piece], h * blk:n * blk, :]
        else:
            src, dst = tab.at[slot, 0:h], tab.at[slot, h:n]
        return pltpu.make_async_remote_copy(
            src, dst, out_sem.at[2 + piece // 2], d_recv.at[slot, piece // 2],
            device_id={"ep": partner}, device_id_type=MESH)

    def d_done(slot, n):
        whole(tok.at[slot, :, n // 2 * blk:n * blk, :], d_recv.at[slot, 0]).wait()
        whole(tab.at[slot, n // 2:n], d_recv.at[slot, 1]).wait()

    def x_copies(slot, n):
        def one(src, dst, to):
            return pltpu.make_async_remote_copy(
                rows.at[slot, 0:n * cap, src], rows.at[slot, 0:n * cap, dst * share:(dst + 1) * share],
                out_sem.at[4], x_recv.at[slot], device_id={"tp": to}, device_id_type=MESH)

        if XS == 2:
            return [one(slice((zs - 1) * share, zs * share), tp - 2, x_left), one(slice(0, share), tp - 1, x_right)]
        if XS == 1:
            return [one(pl.ds(pl.multiple_of((1 - c) * (zs - 1) * share, share), share), tp - 1, x_short)]
        return []

    def rs_copy(slot, n, hop, side):
        top = slice(0, n * cap)
        src = part.at[slot, (hl, tp - hs)[side], top] if hop == 1 else rs.at[slot, hop - 2, side, top]
        return pltpu.make_async_remote_copy(
            src, rs.at[slot, hop - 1, side, top], out_sem.at[5], l_recv.at[slot, hop - 1],
            device_id={"tp": (x_long, x_short)[side]}, device_id_type=MESH)

    def direct_copy(q):
        return pltpu.make_async_remote_copy(
            part.at[last, q, 0:2 * cap], direct.at[tp - q - 1], out_sem.at[6], t_recv.at[0],
            device_id={"tp": wrap(x + q * dl, tp)}, device_id_type=MESH)

    def ret_copy(slot, j, to):
        return pltpu.make_async_remote_copy(
            ret.at[slot, j], results.at[e], out_sem.at[7], r_recv.at[0],
            device_id={"ep": to}, device_id_type=MESH)

    whole(tok_in, in_sem.at[0]).wait()
    whole(gain_in, in_sem.at[1]).wait()
    total = jnp.zeros((blk, 1), F32)
    for q in range(tp):
        value = tok_in[q].astype(F32)
        total = total + jnp.sum(value * value, axis=1, keepdims=True)
    inverse = lax.rsqrt(total / (tp * share) + EPS)

    def norm(q):
        value = tok_in[q].astype(F32) * inverse * gain_in[q]
        tok[mine, q, near, :] = value.astype(BF16)

    for q in range(half):
        norm(q)
    pl.semaphore_wait(barrier, 5)
    z_own(0, 0).start()
    z_own(1, 0).start()
    for q in range(half, zs):
        norm(q)
    z_own(0, 1).start()
    z_own(1, 1).start()
    d_copy(mine, 0, 2).start()
    d_copy(mine, 1, 2).start()

    for copy in second:
        copy.wait()
    expert_ids = lax.broadcasted_iota(I32, (ep, blk), 0)
    hits = jnp.zeros((ep, blk), F32)
    wt = jnp.zeros((ep, blk), F32)
    for k in range(TOP_K):
        hit = routes_in[k:k + 1, :] == expert_ids
        hits = hits + jnp.where(hit, 1.0, 0.0)
        wt = wt + jnp.where(hit, weights_in[k:k + 1, :], 0.0)
    hits_b = hits.astype(BF16)
    row_t = lax.broadcasted_iota(I32, (blk, 2 * blk), 0)
    lane_t = lax.broadcasted_iota(I32, (blk, 2 * blk), 1)
    lane_t = jnp.where(lane_t >= blk, lane_t - blk, lane_t)
    earlier = jnp.where(row_t < lane_t, 1.0, 0.0).astype(BF16)
    same = jnp.where(row_t == lane_t, 1.0, 0.0).astype(BF16)
    slots = jnp.dot(hits_b, same, preferred_element_type=F32) * (
        jnp.dot(hits_b, earlier, preferred_element_type=F32) + 1.0)
    tab[mine, 0] = slots.astype(BF16)
    z_own(0, 2).start()
    z_own(1, 2).start()
    d_copy(mine, 2, 2).start()

    over = (((0,), (0,)), ((), ()))
    slot1 = slots[:, 0:blk].astype(BF16)
    lane = lax.broadcasted_iota(I32, (ep, ep * cap), 1)
    start = lax.broadcasted_iota(I32, (ep, ep * cap), 0) * cap
    inside = jnp.where((lane >= start) & (lane < start + cap), 1.0, 0.0)
    spread = inside.astype(BF16)
    want = jnp.sum(inside * (lane - start + 1).astype(F32), axis=0, keepdims=True)
    wt_hi = wt.astype(BF16)
    wt_lo = (wt - wt_hi.astype(F32)).astype(BF16)
    match = lax.dot_general(slot1, spread, over, preferred_element_type=F32) == want
    c_hi[...] = jnp.where(
        match, lax.dot_general(wt_hi, spread, over, preferred_element_type=F32), 0.0).astype(BF16)
    c_lo[...] = jnp.where(
        match, lax.dot_general(wt_lo, spread, over, preferred_element_type=F32), 0.0).astype(BF16)

    whole(wgu, in_sem.at[5]).wait()
    whole(wd, in_sem.at[6]).wait()

    def arrive(slot, piece):
        @pl.when(slot < last)
        def _():
            z_done(slot, piece, 2).wait()

            @pl.when(slot < last - 1)
            def _():
                z_next(slot, 0, piece).start()
                z_next(slot, 1, piece).start()

            @pl.when(slot == last - 1)
            def _():
                z_end(piece).start()

            d_copy(slot, piece, 4).start()

        @pl.when(slot == last)
        def _():
            z_done(slot, piece, 1).wait()
            d_copy(slot, piece, 2).start()

    left_half = lax.broadcasted_iota(I32, (1, 2 * blk), 1) < blk
    my_expert = lax.broadcasted_iota(I32, (ep, 2 * blk), 0) == e

    def pick(slot, n):
        r_id = lax.broadcasted_iota(I32, (n * cap, n * blk), 0)
        l_id = lax.broadcasted_iota(I32, (n * cap, n * blk), 1)
        my_slot = jnp.full((n * cap, n * blk), -1, I32)
        for j in range(n):
            good = (r_id >= j * cap) & (r_id < (j + 1) * cap) & (l_id >= j * blk) & (l_id < (j + 1) * blk)
            my_slot = jnp.where(good, r_id - j * cap + 1, my_slot)
        d_done(slot, n)
        seen = []
        for j in range(n):
            seen.append(jnp.sum(jnp.where(my_expert, tab[slot, j].astype(F32), 0.0), axis=0, keepdims=True))
        pair = jnp.concatenate(
            [jnp.where(left_half, seen[j], seen[j + 1]) for j in range(0, n, 2)], axis=1)
        choose = jnp.where(my_slot.astype(F32) == pair, 1.0, 0.0).astype(BF16)

        def one(q):
            rows[slot, 0:n * cap, q * share:(q + 1) * share] = jnp.dot(
                choose, tok[slot, q, 0:n * blk, :], preferred_element_type=F32).astype(BF16)

        early = (0, zs - 1) if XS else ()
        for q in early:
            one(q)
        for copy in x_copies(slot, n):
            copy.start()
        for q in range(zs):
            if q not in early:
                one(q)

    def compute(slot, n, ring=True):
        if XS:
            whole(rows.at[slot, 0:n * cap, zs * share:], x_recv.at[slot]).wait()
        acc = jnp.dot(rows[slot, 0:n * cap, :], wgu[...], preferred_element_type=F32)
        gate, up = acc[:, :share], acc[:, share:]
        hidden = (gate / (1.0 + jnp.exp(-gate)) * up).astype(BF16)
        order = sorted(range(tp), key=lambda q: -min(q, tp - q))
        if ring:
            order = [hl, tp - hs] + [q for q in order if q not in (hl, tp - hs)]
        for place, q in enumerate(order):
            part[slot, q, 0:n * cap] = jnp.dot(hidden, wd[q], preferred_element_type=F32).astype(BF16)
            if ring and place < 2:
                rs_copy(slot, n, 1, place).start()
            if not ring and q:
                direct_copy(q).start()

    def hop(slot, n, h):
        top = slice(0, n * cap)
        both = h <= hs
        whole(rs.at[slot, h - 1, :, top] if both else rs.at[slot, h - 1, 0, top], l_recv.at[slot, h - 1]).wait()

        def add(side, q):
            rs[slot, h - 1, side, top] = (
                rs[slot, h - 1, side, top].astype(F32) + part[slot, q, top].astype(F32)).astype(BF16)
            rs_copy(slot, n, h + 1, side).start()

        add(0, hl - h)
        if h < hs:
            add(1, tp - hs + h)

    def give(slot, n, value):
        for j in range(n):
            ret[slot, j] = value[j * cap:(j + 1) * cap].astype(BF16)

    def finish(slot, n):
        top = slice(0, n * cap)
        whole(rs.at[slot, hl - 1, 0, top], l_recv.at[slot, hl - 1]).wait()
        give(slot, n, part[slot, 0, top].astype(F32) + rs[slot, hl - 1, 0, top].astype(F32)
             + rs[slot, hs - 1, 1, top].astype(F32))
        if n == 4:
            for j in range(4):
                ret_copy(slot, j, dev(z + (-1, 1)[j % 2] * (slot + 1), (c, 1 - c)[j // 2])).start()
        else:
            ret_copy(slot, 1, partner).start()
            results[e] = ret[slot, 0]

    def finish_last():
        whole(direct, t_recv.at[0]).wait()
        value = part[last, 0, 0:2 * cap].astype(F32)
        for q in range(tp - 1):
            value = value + direct[q].astype(F32)
        give(last, 2, value)
        ret_copy(last, 0, dev(z + steps, c)).start()
        ret_copy(last, 1, dev(z + steps, 1 - c)).start()

    def at(turn, behind, act):
        @pl.when((turn >= behind) & (turn - behind < last))
        def _():
            act(turn - behind, 4)

        @pl.when(turn - behind == -1)
        def _():
            act(mine, 2)

    def turn(t, carry):
        arrive(t, 0)

        @pl.when((t >= 1) & (t <= last))
        def _():
            pick(t - 1, 4)

        @pl.when(t == steps)
        def _():
            pick(last, 2)

        arrive(t, 1)
        arrive(t, 2)
        at(t, hl + 1, finish)
        for h in range(hl - 1, 0, -1):
            at(t, h + 1, functools.partial(hop, h=h))
        at(t, 1, compute)

        @pl.when(t == steps)
        def _():
            compute(last, 2, False)

        return carry

    pick(mine, 2)
    lax.fori_loop(0, last + hl + 1, turn, 0)
    finish_last()

    whole(results.at[0:ep - 1], r_recv.at[0]).wait()
    got = results[...].astype(F32).reshape(ep * cap, share).astype(BF16)
    combined = jnp.dot(c_hi[...], got, preferred_element_type=F32) + jnp.dot(
        c_lo[...], got, preferred_element_type=F32)
    own_sq = jnp.sum(combined * combined, axis=1, keepdims=True)
    eye = lax.broadcasted_iota(I32, (blk, blk), 0) == lax.broadcasted_iota(I32, (blk, blk), 1)
    flat = jnp.sum(jnp.where(eye, jnp.broadcast_to(own_sq, (blk, blk)), 0.0), axis=0, keepdims=True)
    squares[x] = jnp.broadcast_to(jnp.concatenate([flat, flat], axis=1), squares.shape[1:])

    def q_copy(q):
        return pltpu.make_async_remote_copy(
            squares.at[x], squares.at[x], out_sem.at[8], q_recv.at[0],
            device_id={"tp": wrap(x + q, tp)}, device_id_type=MESH)

    for q in range(1, tp):
        q_copy(q).start()

    def amount(units, most):
        b = max(d for d in range(1, most + 1) if units % d == 0)
        return units // b, b

    a, b = amount(2 * steps - 1, 4)
    whole(tok.at[0:a, :, 0:b * blk, :], out_sem.at[0]).wait()
    whole(tab.at[0:a, 0:b], out_sem.at[1]).wait()
    a, b = amount(2 * steps, 4)
    whole(tok.at[0:a, :, 0:b * blk, :], out_sem.at[2]).wait()
    whole(tab.at[0:a, 0:b], out_sem.at[3]).wait()
    if XS:
        whole(rows.at[0:steps, :, 0:XS * share], out_sem.at[4]).wait()
    a, b = amount((4 * last + 2) * cap // 16, 4 * cap // 16)
    whole(part.at[0:a, 0:tp - 1, 0:b * 16], out_sem.at[5]).wait()
    whole(direct, out_sem.at[6]).wait()
    whole(results.at[0:ep - 1], out_sem.at[7]).wait()
    whole(squares.at[0:tp - 1], out_sem.at[8]).wait()
    whole(squares.at[0:tp - 1], q_recv.at[0]).wait()
    everyone = jnp.sum(squares[...], axis=0)[0:1, 0:blk]
    column = jnp.sum(jnp.where(eye, jnp.broadcast_to(everyone, (blk, blk)), 0.0), axis=1, keepdims=True)
    scale = lax.rsqrt(column / (tp * share) + EPS)
    out[...] = (combined * scale * final_in[...]).astype(out.dtype)


def solution(mesh):
    ep, tp = mesh.shape["ep"], mesh.shape["tp"]

    def per_device(tokens, norm_gain, routes, route_weights, w_gate, w_up, w_down, final_gain):
        blk, features = tokens.shape
        cap = max(2, min(blk, 2 * blk * TOP_K // ep))
        share = features // tp
        slots = ep // CORES // 2 + 1
        hl = tp // 2
        zs = tp - XS
        dma = pltpu.SemaphoreType.DMA
        vmem = pltpu.VMEM
        return pl.pallas_call(
            functools.partial(kernel, ep, tp, cap),
            out_shape=jax.ShapeDtypeStruct((blk, share), BF16),
            in_specs=[pl.BlockSpec(memory_space=pl.ANY)] * 8,
            out_specs=pl.BlockSpec(memory_space=pltpu.VMEM),
            scratch_shapes=[
                vmem((slots, zs, 4 * blk, share), BF16),
                vmem((slots, 4, ep, 2 * blk), BF16),
                vmem((slots, 4 * cap, features), BF16),
                vmem((slots, tp, 4 * cap, share), BF16),
                vmem((slots, hl, 2, 4 * cap, share), BF16),
                vmem((tp - 1, 2 * cap, share), BF16),
                vmem((slots, 4, cap, share), BF16),
                vmem((ep, cap, share), BF16),
                vmem((tp, 8, 2 * blk), F32),
                vmem((tp, blk, share), BF16),
                vmem((tp, 1, share), F32),
                vmem((TOP_K, blk), I32),
                vmem((TOP_K, blk), F32),
                vmem((features, 2 * share), BF16),
                vmem((tp, share, share), BF16),
                vmem((1, share), F32),
                vmem((blk, ep * cap), BF16),
                vmem((blk, ep * cap), BF16),
                dma((7,)), dma((9,)),
                dma((slots - 1, 3)), dma((slots, 2)), dma((slots,)), dma((slots, hl)), dma((1,)), dma((1,)), dma((1,)),
            ],
            compiler_params=pltpu.CompilerParams(
                collective_id=0, has_side_effects=True, vmem_limit_bytes=56 * 1024 * 1024),
        )(tokens, norm_gain.reshape(1, features), routes.T, route_weights.T, w_gate, w_up, w_down,
          final_gain.reshape(1, share))

    placed = (
        P(("grp", "ep"), None),
        P(),
        P(("grp", "ep"), None),
        P(("grp", "ep"), None),
        P("ep", None, "tp"),
        P("ep", None, "tp"),
        P("ep", "tp", None),
        P("tp"),
    )
    return jax.shard_map(
        per_device, mesh=mesh, in_specs=placed, out_specs=P(("grp", "ep"), "tp"), check_vma=False
    )
```

```python
import functools

import jax
import jax.numpy as jnp
from jax import lax
from jax.experimental import pallas as pl
from jax.experimental.pallas import tpu as pltpu
from jax.sharding import PartitionSpec as P

TOP_K = 6
EPS = 1e-06
MESH = pl.DeviceIdType.MESH
BF16, F32, I32 = jnp.bfloat16, jnp.float32, jnp.int32
CORES = 2
XS = 2
PIECES = (2, 2, 2)
Z, PICK, COMP, HOP, FIN = range(5)
ORDER = (
    (PICK, -1), (Z, 0, 0), (COMP, -1), (Z, 0, 1), (Z, 0, 2), (PICK, 0), (Z, 1, 0), (HOP, -1, 1), (Z, 1, 1),
    (Z, 1, 2), (COMP, 0), (Z, 2, 0), (PICK, 1), (HOP, -1, 2), (Z, 2, 1), (Z, 2, 2), (HOP, 0, 1), (PICK, 2),
    (Z, 3, 0), (COMP, 1), (HOP, -1, 3), (Z, 3, 1), (Z, 3, 2), (HOP, 0, 2), (PICK, 3), (Z, 4, 0), (COMP, 2),
    (FIN, -1), (Z, 4, 1), (HOP, 1, 1), (HOP, 0, 3), (Z, 4, 2), (COMP, 3), (Z, 5, 0), (PICK, 4), (HOP, 2, 1),
    (Z, 5, 1), (HOP, 1, 2), (FIN, 0), (Z, 5, 2), (HOP, 3, 1), (PICK, 5), (Z, 6, 0), (COMP, 4), (HOP, 2, 2),
    (Z, 6, 1), (HOP, 1, 3), (Z, 6, 2), (HOP, 3, 2), (Z, 7, 0), (PICK, 6), (COMP, 5), (Z, 7, 1), (HOP, 4, 1),
    (Z, 7, 2), (HOP, 2, 3), (FIN, 1), (PICK, 7), (HOP, 3, 3), (COMP, 6), (HOP, 5, 1), (HOP, 4, 2), (FIN, 2),
    (COMP, 7), (FIN, 3), (HOP, 6, 1), (HOP, 5, 2), (HOP, 4, 3), (HOP, 7, 1), (HOP, 6, 2), (HOP, 5, 3), (FIN, 4),
    (HOP, 7, 2), (HOP, 6, 3), (FIN, 5), (HOP, 7, 3), (FIN, 6), (FIN, 7),
)


def wrap(value, count):
    return lax.rem(value + 4 * count, count)


def kernel(
    ep, tp, cap,
    tokens, norm_gain, routes, route_weights, w_gate, w_up, w_down, final_gain,
    out,
    tok, tab, rows, part, rs, ret, results, squares,
    tok_in, gain_in, routes_in, weights_in, wgu, wd, final_in, c_hi, c_lo,
    in_sem, out_sem, z_recv, d_recv, x_recv, l_recv, r_recv, q_recv,
):
    e = lax.axis_index("ep")
    x = lax.axis_index("tp")
    z, c = lax.div(e, CORES), lax.rem(e, CORES)
    nz = ep // CORES
    steps = nz // 2
    zs = tp - XS
    back = (zs - 1) // 2
    hl, hs = tp // 2, tp - 1 - tp // 2
    blk = tok_in.shape[1]
    share = tok_in.shape[2]
    last, mine = steps - 1, steps
    cuts = [sum(PIECES[:p]) for p in range(len(PIECES) + 1)]
    np_ = len(PIECES)

    def dev(zz, cc):
        return wrap(zz, nz) * CORES + cc

    up_z, down_z, partner = dev(z + 1, c), dev(z - 1, c), dev(z, 1 - c)
    x_right, x_left = wrap(x + 1, tp), wrap(x - 1, tp)
    dl = 1 - 2 * c
    x_long, x_short = wrap(x + dl, tp), wrap(x - dl, tp)

    barrier = pltpu.get_barrier_semaphore()
    for who in ({"ep": up_z}, {"ep": down_z}, {"ep": partner}, {"tp": x_right}, {"tp": x_left}):
        pl.semaphore_signal(barrier, inc=1, device_id=who, device_id_type=MESH)

    def lanes(q):
        return pl.ds(pl.multiple_of(wrap(x - back + q, tp) * share, share), share)

    for q in range(tp):
        pltpu.make_async_copy(tokens.at[:, lanes(q)], tok_in.at[q], in_sem.at[0]).start()
        pltpu.make_async_copy(norm_gain.at[:, lanes(q)], gain_in.at[q], in_sem.at[1]).start()
    second = [pltpu.make_async_copy(routes, routes_in, in_sem.at[2]),
              pltpu.make_async_copy(route_weights, weights_in, in_sem.at[3]),
              pltpu.make_async_copy(final_gain, final_in, in_sem.at[4])]
    for copy in second:
        copy.start()
    for q in range(tp):
        rows_q = slice(q * share, (q + 1) * share)
        pltpu.make_async_copy(w_gate.at[0, lanes(q), :], wgu.at[rows_q, 0:share], in_sem.at[5]).start()
        pltpu.make_async_copy(w_up.at[0, lanes(q), :], wgu.at[rows_q, share:2 * share], in_sem.at[5]).start()
        owner = pl.ds(pl.multiple_of(wrap(x + q * dl, tp) * share, share), share)
        pltpu.make_async_copy(w_down.at[0, :, owner], wd.at[q], in_sem.at[6]).start()

    def whole(ref, sem):
        return pltpu.make_async_copy(ref, ref, sem)

    near, far = slice(0, blk), slice(blk, 2 * blk)
    halves = [slice(a, b) for a, b in zip(cuts, cuts[1:])]

    def z_copy(dst_slot, piece, to, src_slot, src_tok, src_tab, dst_tok, dst_tab):
        if piece < np_:
            src, dst = tok.at[src_slot, halves[piece], src_tok, :], tok.at[dst_slot, halves[piece], dst_tok, :]
        else:
            src, dst = tab.at[src_slot, src_tab], tab.at[dst_slot, dst_tab]
        return pltpu.make_async_remote_copy(
            src, dst, out_sem.at[piece // np_], z_recv.at[dst_slot, piece],
            device_id={"ep": to}, device_id_type=MESH)

    def z_own(way, piece):
        return z_copy(0, piece, (up_z, down_z)[way], mine, near, 0, (near, far)[way], way)

    def z_next(slot, way, piece):
        where = (near, far)[way]
        return z_copy(slot + 1, piece, (up_z, down_z)[way], slot, where, way, where, way)

    def z_end(piece):
        there = pl.ds(pl.multiple_of(c * blk, blk), blk)
        return z_copy(last, piece, jnp.where(c == 0, up_z, down_z), last - 1, there, c, near, 0)

    def z_done(slot, piece, n):
        ref = tok.at[slot, halves[piece], 0:n * blk, :] if piece < np_ else tab.at[slot, 0:n]
        return whole(ref, z_recv.at[slot, piece])

    def d_copy(slot, piece, n):
        h = n // 2
        if piece < np_:
            src = tok.at[slot, halves[piece], 0:h * blk, :]
            dst = tok.at[slot, halves[piece], h * blk:n * blk, :]
        else:
            src, dst = tab.at[slot, 0:h], tab.at[slot, h:n]
        return pltpu.make_async_remote_copy(
            src, dst, out_sem.at[2 + piece // np_], d_recv.at[slot, piece // np_],
            device_id={"ep": partner}, device_id_type=MESH)

    def d_done(slot, n):
        whole(tok.at[slot, :, n // 2 * blk:n * blk, :], d_recv.at[slot, 0]).wait()
        whole(tab.at[slot, n // 2:n], d_recv.at[slot, 1]).wait()

    def x_copies(slot, n):
        def one(src, dst, to):
            return pltpu.make_async_remote_copy(
                rows.at[slot, 0:n * cap, src], rows.at[slot, 0:n * cap, dst * share:(dst + 1) * share],
                out_sem.at[4], x_recv.at[slot], device_id={"tp": to}, device_id_type=MESH)

        if XS == 2:
            return [one(slice((zs - 1) * share, zs * share), tp - 2, x_left), one(slice(0, share), tp - 1, x_right)]
        if XS == 1:
            return [one(pl.ds(pl.multiple_of((1 - c) * (zs - 1) * share, share), share), tp - 1, x_short)]
        return []

    def rs_copy(slot, n, hop, side):
        top = slice(0, n * cap)
        src = part.at[slot, (hl, tp - hs)[side], top] if hop == 1 else rs.at[slot, hop - 2, side, top]
        return pltpu.make_async_remote_copy(
            src, rs.at[slot, hop - 1, side, top], out_sem.at[5], l_recv.at[slot, hop - 1],
            device_id={"tp": (x_long, x_short)[side]}, device_id_type=MESH)

    def ret_copy(slot, j, to):
        return pltpu.make_async_remote_copy(
            ret.at[slot, j], results.at[e], out_sem.at[7], r_recv.at[0],
            device_id={"ep": to}, device_id_type=MESH)

    whole(tok_in, in_sem.at[0]).wait()
    whole(gain_in, in_sem.at[1]).wait()
    total = jnp.zeros((blk, 1), F32)
    for q in range(tp):
        value = tok_in[q].astype(F32)
        total = total + jnp.sum(value * value, axis=1, keepdims=True)
    inverse = lax.rsqrt(total / (tp * share) + EPS)

    def norm(q):
        value = tok_in[q].astype(F32) * inverse * gain_in[q]
        tok[mine, q, near, :] = value.astype(BF16)

    for p in range(np_):
        for q in range(cuts[p], cuts[p + 1]):
            norm(q)
        if p == 0:
            pl.semaphore_wait(barrier, 5)
        z_own(0, p).start()
        z_own(1, p).start()
    for p in range(np_):
        d_copy(mine, p, 2).start()

    for copy in second:
        copy.wait()
    expert_ids = lax.broadcasted_iota(I32, (ep, blk), 0)
    hits = jnp.zeros((ep, blk), F32)
    wt = jnp.zeros((ep, blk), F32)
    for k in range(TOP_K):
        hit = routes_in[k:k + 1, :] == expert_ids
        hits = hits + jnp.where(hit, 1.0, 0.0)
        wt = wt + jnp.where(hit, weights_in[k:k + 1, :], 0.0)
    hits_b = hits.astype(BF16)
    row_t = lax.broadcasted_iota(I32, (blk, 2 * blk), 0)
    lane_t = lax.broadcasted_iota(I32, (blk, 2 * blk), 1)
    lane_t = jnp.where(lane_t >= blk, lane_t - blk, lane_t)
    earlier = jnp.where(row_t < lane_t, 1.0, 0.0).astype(BF16)
    same = jnp.where(row_t == lane_t, 1.0, 0.0).astype(BF16)
    slots = jnp.dot(hits_b, same, preferred_element_type=F32) * (
        jnp.dot(hits_b, earlier, preferred_element_type=F32) + 1.0)
    tab[mine, 0] = slots.astype(BF16)
    z_own(0, np_).start()
    z_own(1, np_).start()
    d_copy(mine, np_, 2).start()

    over = (((0,), (0,)), ((), ()))
    slot1 = slots[:, 0:blk].astype(BF16)
    lane = lax.broadcasted_iota(I32, (ep, ep * cap), 1)
    start = lax.broadcasted_iota(I32, (ep, ep * cap), 0) * cap
    inside = jnp.where((lane >= start) & (lane < start + cap), 1.0, 0.0)
    spread = inside.astype(BF16)
    want = jnp.sum(inside * (lane - start + 1).astype(F32), axis=0, keepdims=True)
    wt_hi = wt.astype(BF16)
    wt_lo = (wt - wt_hi.astype(F32)).astype(BF16)
    match = lax.dot_general(slot1, spread, over, preferred_element_type=F32) == want
    c_hi[...] = jnp.where(
        match, lax.dot_general(wt_hi, spread, over, preferred_element_type=F32), 0.0).astype(BF16)
    c_lo[...] = jnp.where(
        match, lax.dot_general(wt_lo, spread, over, preferred_element_type=F32), 0.0).astype(BF16)

    whole(wgu, in_sem.at[5]).wait()
    whole(wd, in_sem.at[6]).wait()

    def arrive(slot, piece):
        n = 4 if slot < last else 2
        z_done(slot, piece, n // 2).wait()
        if slot < last - 1:
            z_next(slot, 0, piece).start()
            z_next(slot, 1, piece).start()
        elif slot == last - 1:
            z_end(piece).start()
        d_copy(slot, piece, n).start()

    left_half = lax.broadcasted_iota(I32, (1, 2 * blk), 1) < blk
    my_expert = lax.broadcasted_iota(I32, (ep, 2 * blk), 0) == e

    def pick(slot, n):
        r_id = lax.broadcasted_iota(I32, (n * cap, n * blk), 0)
        l_id = lax.broadcasted_iota(I32, (n * cap, n * blk), 1)
        my_slot = jnp.full((n * cap, n * blk), -1, I32)
        for j in range(n):
            good = (r_id >= j * cap) & (r_id < (j + 1) * cap) & (l_id >= j * blk) & (l_id < (j + 1) * blk)
            my_slot = jnp.where(good, r_id - j * cap + 1, my_slot)
        d_done(slot, n)
        seen = []
        for j in range(n):
            seen.append(jnp.sum(jnp.where(my_expert, tab[slot, j].astype(F32), 0.0), axis=0, keepdims=True))
        pair = jnp.concatenate(
            [jnp.where(left_half, seen[j], seen[j + 1]) for j in range(0, n, 2)], axis=1)
        choose = jnp.where(my_slot.astype(F32) == pair, 1.0, 0.0).astype(BF16)

        def one(q):
            rows[slot, 0:n * cap, q * share:(q + 1) * share] = jnp.dot(
                choose, tok[slot, q, 0:n * blk, :], preferred_element_type=F32).astype(BF16)

        early = (0, zs - 1) if XS else ()
        for q in early:
            one(q)
        for copy in x_copies(slot, n):
            copy.start()
        for q in range(zs):
            if q not in early:
                one(q)

    def compute(slot, n):
        whole(rows.at[slot, 0:n * cap, zs * share:], x_recv.at[slot]).wait()
        acc = jnp.dot(rows[slot, 0:n * cap, :], wgu[...], preferred_element_type=F32)
        gate, up = acc[:, :share], acc[:, share:]
        hidden = (gate / (1.0 + jnp.exp(-gate)) * up).astype(BF16)
        order = [hl, tp - hs] + [q for q in range(tp) if q not in (hl, tp - hs)]
        for place, q in enumerate(order):
            part[slot, q, 0:n * cap] = jnp.dot(hidden, wd[q], preferred_element_type=F32).astype(BF16)
            if place < 2:
                rs_copy(slot, n, 1, place).start()

    def hop(slot, n, h):
        top = slice(0, n * cap)
        both = h <= hs
        whole(rs.at[slot, h - 1, :, top] if both else rs.at[slot, h - 1, 0, top], l_recv.at[slot, h - 1]).wait()

        def add(side, q):
            rs[slot, h - 1, side, top] = (
                rs[slot, h - 1, side, top].astype(F32) + part[slot, q, top].astype(F32)).astype(BF16)
            rs_copy(slot, n, h + 1, side).start()

        add(0, hl - h)
        if h < hs:
            add(1, tp - hs + h)

    def give(slot, n, value):
        for j in range(n):
            ret[slot, j] = value[j * cap:(j + 1) * cap].astype(BF16)

    def finish(slot, n):
        top = slice(0, n * cap)
        whole(rs.at[slot, hl - 1, 0, top], l_recv.at[slot, hl - 1]).wait()
        give(slot, n, part[slot, 0, top].astype(F32) + rs[slot, hl - 1, 0, top].astype(F32)
             + rs[slot, hs - 1, 1, top].astype(F32))
        if slot == mine:
            ret_copy(slot, 1, partner).start()
            results[e] = ret[slot, 0]
        elif slot == last:
            ret_copy(slot, 0, dev(z + steps, c)).start()
            ret_copy(slot, 1, dev(z + steps, 1 - c)).start()
        else:
            for j in range(4):
                ret_copy(slot, j, dev(z + (-1, 1)[j % 2] * (slot + 1), (c, 1 - c)[j // 2])).start()

    for kind, chunk, *which in ORDER:
        slot = chunk if chunk >= 0 else mine
        n = 2 if slot >= last else 4
        if kind == Z:
            arrive(slot, *which)
            if which[0] == np_ - 1:
                arrive(slot, np_)
        else:
            (pick, compute, hop, finish)[kind - PICK](slot, n, *which)

    whole(results.at[0:ep - 1], r_recv.at[0]).wait()
    got = results[...].astype(F32).reshape(ep * cap, share).astype(BF16)
    combined = jnp.dot(c_hi[...], got, preferred_element_type=F32) + jnp.dot(
        c_lo[...], got, preferred_element_type=F32)
    own_sq = jnp.sum(combined * combined, axis=1, keepdims=True)
    eye = lax.broadcasted_iota(I32, (blk, blk), 0) == lax.broadcasted_iota(I32, (blk, blk), 1)
    flat = jnp.sum(jnp.where(eye, jnp.broadcast_to(own_sq, (blk, blk)), 0.0), axis=0, keepdims=True)
    squares[x] = jnp.broadcast_to(jnp.concatenate([flat, flat], axis=1), squares.shape[1:])

    def q_copy(q):
        return pltpu.make_async_remote_copy(
            squares.at[x], squares.at[x], out_sem.at[8], q_recv.at[0],
            device_id={"tp": wrap(x + q, tp)}, device_id_type=MESH)

    for q in range(1, tp):
        q_copy(q).start()

    def amount(units, most):
        b = max(d for d in range(1, most + 1) if units % d == 0)
        return units // b, b

    a, b = amount(2 * steps - 1, 4)
    whole(tok.at[0:a, :, 0:b * blk, :], out_sem.at[0]).wait()
    whole(tab.at[0:a, 0:b], out_sem.at[1]).wait()
    a, b = amount(2 * steps, 4)
    whole(tok.at[0:a, :, 0:b * blk, :], out_sem.at[2]).wait()
    whole(tab.at[0:a, 0:b], out_sem.at[3]).wait()
    if XS:
        whole(rows.at[0:steps, :, 0:XS * share], out_sem.at[4]).wait()
    whole(part.at[0:steps, 0:tp - 1], out_sem.at[5]).wait()
    whole(results.at[0:ep - 1], out_sem.at[7]).wait()
    whole(squares.at[0:tp - 1], out_sem.at[8]).wait()
    whole(squares.at[0:tp - 1], q_recv.at[0]).wait()
    everyone = jnp.sum(squares[...], axis=0)[0:1, 0:blk]
    column = jnp.sum(jnp.where(eye, jnp.broadcast_to(everyone, (blk, blk)), 0.0), axis=1, keepdims=True)
    scale = lax.rsqrt(column / (tp * share) + EPS)
    out[...] = (combined * scale * final_in[...]).astype(out.dtype)


def solution(mesh):
    ep, tp = mesh.shape["ep"], mesh.shape["tp"]

    def per_device(tokens, norm_gain, routes, route_weights, w_gate, w_up, w_down, final_gain):
        blk, features = tokens.shape
        cap = max(2, min(blk, 2 * blk * TOP_K // ep))
        share = features // tp
        slots = ep // CORES // 2 + 1
        hl = tp // 2
        zs = tp - XS
        dma = pltpu.SemaphoreType.DMA
        vmem = pltpu.VMEM
        return pl.pallas_call(
            functools.partial(kernel, ep, tp, cap),
            out_shape=jax.ShapeDtypeStruct((blk, share), BF16),
            in_specs=[pl.BlockSpec(memory_space=pl.ANY)] * 8,
            out_specs=pl.BlockSpec(memory_space=pltpu.VMEM),
            scratch_shapes=[
                vmem((slots, zs, 4 * blk, share), BF16),
                vmem((slots, 4, ep, 2 * blk), BF16),
                vmem((slots, 4 * cap, features), BF16),
                vmem((slots, tp, 4 * cap, share), BF16),
                vmem((slots, hl, 2, 4 * cap, share), BF16),
                vmem((slots, 4, cap, share), BF16),
                vmem((ep, cap, share), BF16),
                vmem((tp, 8, 2 * blk), F32),
                vmem((tp, blk, share), BF16),
                vmem((tp, 1, share), F32),
                vmem((TOP_K, blk), I32),
                vmem((TOP_K, blk), F32),
                vmem((features, 2 * share), BF16),
                vmem((tp, share, share), BF16),
                vmem((1, share), F32),
                vmem((blk, ep * cap), BF16),
                vmem((blk, ep * cap), BF16),
                dma((7,)), dma((9,)),
                dma((slots - 1, len(PIECES) + 1)), dma((slots, 2)), dma((slots,)), dma((slots, hl)), dma((1,)), dma((1,)),
            ],
            compiler_params=pltpu.CompilerParams(
                collective_id=0, has_side_effects=True, vmem_limit_bytes=56 * 1024 * 1024),
        )(tokens, norm_gain.reshape(1, features), routes.T, route_weights.T, w_gate, w_up, w_down,
          final_gain.reshape(1, share))

    placed = (
        P(("grp", "ep"), None),
        P(),
        P(("grp", "ep"), None),
        P(("grp", "ep"), None),
        P("ep", None, "tp"),
        P("ep", None, "tp"),
        P("ep", "tp", None),
        P("tp"),
    )
    return jax.shard_map(
        per_device, mesh=mesh, in_specs=placed, out_specs=P(("grp", "ep"), "tp"), check_vma=False
    )
```

```python
import functools

import jax
import jax.numpy as jnp
from jax import lax
from jax.experimental import pallas as pl
from jax.experimental.pallas import tpu as pltpu
from jax.sharding import PartitionSpec as P

TOP_K = 6
EPS = 1e-06
MESH = pl.DeviceIdType.MESH
BF16, F32, I32 = jnp.bfloat16, jnp.float32, jnp.int32
CORES = 2
XS = 2
PIECES = (2, 2, 2)
Z, PICK, COMP, HOP, FIN = range(5)
ORDER = (
    (PICK, -1), (Z, 0, 0), (COMP, -1), (Z, 0, 1), (Z, 0, 2), (PICK, 0), (Z, 1, 0), (HOP, -1, 1), (Z, 1, 1),
    (Z, 1, 2), (COMP, 0), (Z, 2, 0), (PICK, 1), (HOP, -1, 2), (Z, 2, 1), (Z, 2, 2), (HOP, 0, 1), (PICK, 2),
    (Z, 3, 0), (COMP, 1), (HOP, -1, 3), (Z, 3, 1), (Z, 3, 2), (HOP, 0, 2), (PICK, 3), (Z, 4, 0), (COMP, 2),
    (FIN, -1), (Z, 4, 1), (HOP, 1, 1), (HOP, 0, 3), (Z, 4, 2), (COMP, 3), (Z, 5, 0), (PICK, 4), (HOP, 2, 1),
    (Z, 5, 1), (HOP, 1, 2), (FIN, 0), (Z, 5, 2), (HOP, 3, 1), (PICK, 5), (Z, 6, 0), (COMP, 4), (HOP, 2, 2),
    (Z, 6, 1), (HOP, 1, 3), (Z, 6, 2), (HOP, 3, 2), (Z, 7, 0), (PICK, 6), (COMP, 5), (Z, 7, 1), (HOP, 4, 1),
    (Z, 7, 2), (HOP, 2, 3), (FIN, 1), (PICK, 7), (HOP, 3, 3), (COMP, 6), (HOP, 5, 1), (HOP, 4, 2), (FIN, 2),
    (COMP, 7), (FIN, 3), (HOP, 6, 1), (HOP, 5, 2), (HOP, 4, 3), (HOP, 7, 1), (HOP, 6, 2), (HOP, 5, 3), (FIN, 4),
    (HOP, 7, 2), (HOP, 6, 3), (FIN, 5), (HOP, 7, 3), (FIN, 6), (FIN, 7),
)


def wrap(value, count):
    return lax.rem(value + 4 * count, count)


def kernel(
    ep, tp, cap,
    tokens, norm_gain, routes, route_weights, w_gate, w_up, w_down, final_gain,
    out,
    tok, tab, rows, part, rs, ret, results, late, squares,
    tok_in, gain_in, routes_in, weights_in, wgu, wd, final_in, c_hi, c_lo, cl_hi, cl_lo,
    in_sem, out_sem, z_recv, d_recv, x_recv, l_recv, r_recv, q_recv,
):
    e = lax.axis_index("ep")
    x = lax.axis_index("tp")
    z, c = lax.div(e, CORES), lax.rem(e, CORES)
    nz = ep // CORES
    steps = nz // 2
    zs = tp - XS
    back = (zs - 1) // 2
    hl, hs = tp // 2, tp - 1 - tp // 2
    blk = tok_in.shape[1]
    share = tok_in.shape[2]
    last, mine = steps - 1, steps
    cuts = [sum(PIECES[:p]) for p in range(len(PIECES) + 1)]
    np_ = len(PIECES)

    def dev(zz, cc):
        return wrap(zz, nz) * CORES + cc

    up_z, down_z, partner = dev(z + 1, c), dev(z - 1, c), dev(z, 1 - c)
    x_right, x_left = wrap(x + 1, tp), wrap(x - 1, tp)
    dl = 1 - 2 * c
    x_long, x_short = wrap(x + dl, tp), wrap(x - dl, tp)

    barrier = pltpu.get_barrier_semaphore()
    for who in ({"ep": up_z}, {"ep": down_z}, {"ep": partner}, {"tp": x_right}, {"tp": x_left}):
        pl.semaphore_signal(barrier, inc=1, device_id=who, device_id_type=MESH)

    def lanes(q):
        return pl.ds(pl.multiple_of(wrap(x - back + q, tp) * share, share), share)

    for q in range(tp):
        pltpu.make_async_copy(tokens.at[:, lanes(q)], tok_in.at[q], in_sem.at[0]).start()
        pltpu.make_async_copy(norm_gain.at[:, lanes(q)], gain_in.at[q], in_sem.at[1]).start()
    second = [pltpu.make_async_copy(routes, routes_in, in_sem.at[2]),
              pltpu.make_async_copy(route_weights, weights_in, in_sem.at[3]),
              pltpu.make_async_copy(final_gain, final_in, in_sem.at[4])]
    for copy in second:
        copy.start()
    for q in range(tp):
        rows_q = slice(q * share, (q + 1) * share)
        pltpu.make_async_copy(w_gate.at[0, lanes(q), :], wgu.at[rows_q, 0:share], in_sem.at[5]).start()
        pltpu.make_async_copy(w_up.at[0, lanes(q), :], wgu.at[rows_q, share:2 * share], in_sem.at[5]).start()
        owner = pl.ds(pl.multiple_of(wrap(x + q * dl, tp) * share, share), share)
        pltpu.make_async_copy(w_down.at[0, :, owner], wd.at[q], in_sem.at[6]).start()

    def whole(ref, sem):
        return pltpu.make_async_copy(ref, ref, sem)

    near, far = slice(0, blk), slice(blk, 2 * blk)
    halves = [slice(a, b) for a, b in zip(cuts, cuts[1:])]

    def z_copy(dst_slot, piece, to, src_slot, src_tok, src_tab, dst_tok, dst_tab):
        if piece < np_:
            src, dst = tok.at[src_slot, halves[piece], src_tok, :], tok.at[dst_slot, halves[piece], dst_tok, :]
        else:
            src, dst = tab.at[src_slot, src_tab], tab.at[dst_slot, dst_tab]
        return pltpu.make_async_remote_copy(
            src, dst, out_sem.at[piece // np_], z_recv.at[dst_slot, piece],
            device_id={"ep": to}, device_id_type=MESH)

    def z_own(way, piece):
        return z_copy(0, piece, (up_z, down_z)[way], mine, near, 0, (near, far)[way], way)

    def z_next(slot, way, piece):
        where = (near, far)[way]
        return z_copy(slot + 1, piece, (up_z, down_z)[way], slot, where, way, where, way)

    def z_end(piece):
        there = pl.ds(pl.multiple_of(c * blk, blk), blk)
        return z_copy(last, piece, jnp.where(c == 0, up_z, down_z), last - 1, there, c, near, 0)

    def z_done(slot, piece, n):
        ref = tok.at[slot, halves[piece], 0:n * blk, :] if piece < np_ else tab.at[slot, 0:n]
        return whole(ref, z_recv.at[slot, piece])

    def d_copy(slot, piece, n):
        h = n // 2
        if piece < np_:
            src = tok.at[slot, halves[piece], 0:h * blk, :]
            dst = tok.at[slot, halves[piece], h * blk:n * blk, :]
        else:
            src, dst = tab.at[slot, 0:h], tab.at[slot, h:n]
        return pltpu.make_async_remote_copy(
            src, dst, out_sem.at[2 + piece // np_], d_recv.at[slot, piece // np_],
            device_id={"ep": partner}, device_id_type=MESH)

    def d_done(slot, n):
        whole(tok.at[slot, :, n // 2 * blk:n * blk, :], d_recv.at[slot, 0]).wait()
        whole(tab.at[slot, n // 2:n], d_recv.at[slot, 1]).wait()

    def x_copies(slot, n):
        def one(src, dst, to):
            return pltpu.make_async_remote_copy(
                rows.at[slot, 0:n * cap, src], rows.at[slot, 0:n * cap, dst * share:(dst + 1) * share],
                out_sem.at[4], x_recv.at[slot], device_id={"tp": to}, device_id_type=MESH)

        if XS == 2:
            return [one(slice((zs - 1) * share, zs * share), tp - 2, x_left), one(slice(0, share), tp - 1, x_right)]
        if XS == 1:
            return [one(pl.ds(pl.multiple_of((1 - c) * (zs - 1) * share, share), share), tp - 1, x_short)]
        return []

    def rs_copy(slot, n, hop, side):
        top = slice(0, n * cap)
        src = part.at[slot, (hl, tp - hs)[side], top] if hop == 1 else rs.at[slot, hop - 2, side, top]
        return pltpu.make_async_remote_copy(
            src, rs.at[slot, hop - 1, side, top], out_sem.at[5], l_recv.at[slot, hop - 1],
            device_id={"tp": (x_long, x_short)[side]}, device_id_type=MESH)

    def ret_copy(slot, j, to):
        dst, sem = (late.at[c], r_recv.at[1]) if slot == last else (results.at[e], r_recv.at[0])
        return pltpu.make_async_remote_copy(
            ret.at[slot, j], dst, out_sem.at[7], sem, device_id={"ep": to}, device_id_type=MESH)

    whole(tok_in, in_sem.at[0]).wait()
    whole(gain_in, in_sem.at[1]).wait()
    total = jnp.zeros((blk, 1), F32)
    for q in range(tp):
        value = tok_in[q].astype(F32)
        total = total + jnp.sum(value * value, axis=1, keepdims=True)
    inverse = lax.rsqrt(total / (tp * share) + EPS)

    def norm(q):
        value = tok_in[q].astype(F32) * inverse * gain_in[q]
        tok[mine, q, near, :] = value.astype(BF16)

    for p in range(np_):
        for q in range(cuts[p], cuts[p + 1]):
            norm(q)
        if p == 0:
            pl.semaphore_wait(barrier, 5)
        z_own(0, p).start()
        z_own(1, p).start()
    for p in range(np_):
        d_copy(mine, p, 2).start()

    for copy in second:
        copy.wait()
    expert_ids = lax.broadcasted_iota(I32, (ep, blk), 0)
    hits = jnp.zeros((ep, blk), F32)
    wt = jnp.zeros((ep, blk), F32)
    for k in range(TOP_K):
        hit = routes_in[k:k + 1, :] == expert_ids
        hits = hits + jnp.where(hit, 1.0, 0.0)
        wt = wt + jnp.where(hit, weights_in[k:k + 1, :], 0.0)
    hits_b = hits.astype(BF16)
    row_t = lax.broadcasted_iota(I32, (blk, 2 * blk), 0)
    lane_t = lax.broadcasted_iota(I32, (blk, 2 * blk), 1)
    lane_t = jnp.where(lane_t >= blk, lane_t - blk, lane_t)
    earlier = jnp.where(row_t < lane_t, 1.0, 0.0).astype(BF16)
    same = jnp.where(row_t == lane_t, 1.0, 0.0).astype(BF16)
    slots = jnp.dot(hits_b, same, preferred_element_type=F32) * (
        jnp.dot(hits_b, earlier, preferred_element_type=F32) + 1.0)
    tab[mine, 0] = slots.astype(BF16)
    z_own(0, np_).start()
    z_own(1, np_).start()
    d_copy(mine, np_, 2).start()

    over = (((0,), (0,)), ((), ()))
    slot1 = slots[:, 0:blk].astype(BF16)
    wt_hi = wt.astype(BF16)
    wt_lo = (wt - wt_hi.astype(F32)).astype(BF16)

    def put_together(first, count, hi, lo):
        lane = lax.broadcasted_iota(I32, (ep, count * cap), 1)
        start = (lax.broadcasted_iota(I32, (ep, count * cap), 0) - first) * cap
        inside = jnp.where((lane >= start) & (lane < start + cap), 1.0, 0.0)
        spread = inside.astype(BF16)
        want = jnp.sum(inside * (lane - start + 1).astype(F32), axis=0, keepdims=True)
        match = lax.dot_general(slot1, spread, over, preferred_element_type=F32) == want
        for weight, ref in ((wt_hi, hi), (wt_lo, lo)):
            value = lax.dot_general(weight, spread, over, preferred_element_type=F32)
            ref[...] = jnp.where(match, value, 0.0).astype(BF16)

    opposite = dev(z + steps, 0)
    put_together(0, ep, c_hi, c_lo)
    put_together(opposite, CORES, cl_hi, cl_lo)
    results[pl.ds(opposite, CORES)] = jnp.zeros((CORES, cap, share), BF16)

    whole(wgu, in_sem.at[5]).wait()
    whole(wd, in_sem.at[6]).wait()

    def arrive(slot, piece):
        n = 4 if slot < last else 2
        z_done(slot, piece, n // 2).wait()
        if slot < last - 1:
            z_next(slot, 0, piece).start()
            z_next(slot, 1, piece).start()
        elif slot == last - 1:
            z_end(piece).start()
        d_copy(slot, piece, n).start()

    left_half = lax.broadcasted_iota(I32, (1, 2 * blk), 1) < blk
    my_expert = lax.broadcasted_iota(I32, (ep, 2 * blk), 0) == e

    def pick(slot, n):
        r_id = lax.broadcasted_iota(I32, (n * cap, n * blk), 0)
        l_id = lax.broadcasted_iota(I32, (n * cap, n * blk), 1)
        my_slot = jnp.full((n * cap, n * blk), -1, I32)
        for j in range(n):
            good = (r_id >= j * cap) & (r_id < (j + 1) * cap) & (l_id >= j * blk) & (l_id < (j + 1) * blk)
            my_slot = jnp.where(good, r_id - j * cap + 1, my_slot)
        d_done(slot, n)
        seen = []
        for j in range(n):
            seen.append(jnp.sum(jnp.where(my_expert, tab[slot, j].astype(F32), 0.0), axis=0, keepdims=True))
        pair = jnp.concatenate(
            [jnp.where(left_half, seen[j], seen[j + 1]) for j in range(0, n, 2)], axis=1)
        choose = jnp.where(my_slot.astype(F32) == pair, 1.0, 0.0).astype(BF16)

        def one(q):
            rows[slot, 0:n * cap, q * share:(q + 1) * share] = jnp.dot(
                choose, tok[slot, q, 0:n * blk, :], preferred_element_type=F32).astype(BF16)

        early = (0, zs - 1) if XS else ()
        for q in early:
            one(q)
        for copy in x_copies(slot, n):
            copy.start()
        for q in range(zs):
            if q not in early:
                one(q)

    def compute(slot, n):
        whole(rows.at[slot, 0:n * cap, zs * share:], x_recv.at[slot]).wait()
        acc = jnp.dot(rows[slot, 0:n * cap, :], wgu[...], preferred_element_type=F32)
        gate, up = acc[:, :share], acc[:, share:]
        hidden = (gate / (1.0 + jnp.exp(-gate)) * up).astype(BF16)
        order = [hl, tp - hs] + [q for q in range(tp) if q not in (hl, tp - hs)]
        for place, q in enumerate(order):
            part[slot, q, 0:n * cap] = jnp.dot(hidden, wd[q], preferred_element_type=F32).astype(BF16)
            if place < 2:
                rs_copy(slot, n, 1, place).start()

    def hop(slot, n, h):
        top = slice(0, n * cap)
        both = h <= hs
        whole(rs.at[slot, h - 1, :, top] if both else rs.at[slot, h - 1, 0, top], l_recv.at[slot, h - 1]).wait()

        def add(side, q):
            rs[slot, h - 1, side, top] = (
                rs[slot, h - 1, side, top].astype(F32) + part[slot, q, top].astype(F32)).astype(BF16)
            rs_copy(slot, n, h + 1, side).start()

        add(0, hl - h)
        if h < hs:
            add(1, tp - hs + h)

    def give(slot, n, value):
        for j in range(n):
            ret[slot, j] = value[j * cap:(j + 1) * cap].astype(BF16)

    def finish(slot, n):
        top = slice(0, n * cap)
        whole(rs.at[slot, hl - 1, 0, top], l_recv.at[slot, hl - 1]).wait()
        give(slot, n, part[slot, 0, top].astype(F32) + rs[slot, hl - 1, 0, top].astype(F32)
             + rs[slot, hs - 1, 1, top].astype(F32))
        if slot == mine:
            ret_copy(slot, 1, partner).start()
            results[e] = ret[slot, 0]
        elif slot == last:
            ret_copy(slot, 0, dev(z + steps, c)).start()
            ret_copy(slot, 1, dev(z + steps, 1 - c)).start()
        else:
            for j in range(4):
                ret_copy(slot, j, dev(z + (-1, 1)[j % 2] * (slot + 1), (c, 1 - c)[j // 2])).start()

    for kind, chunk, *which in ORDER:
        slot = chunk if chunk >= 0 else mine
        n = 2 if slot >= last else 4
        if kind == Z:
            arrive(slot, *which)
            if which[0] == np_ - 1:
                arrive(slot, np_)
        else:
            (pick, compute, hop, finish)[kind - PICK](slot, n, *which)

    def weigh(ref, hi, lo):
        got = ref[...].astype(F32).reshape(-1, share).astype(BF16)
        return jnp.dot(hi[...], got, preferred_element_type=F32) + jnp.dot(
            lo[...], got, preferred_element_type=F32)

    whole(results.at[0:ep - 1 - CORES], r_recv.at[0]).wait()
    combined = weigh(results, c_hi, c_lo)
    whole(late, r_recv.at[1]).wait()
    combined = combined + weigh(late, cl_hi, cl_lo)
    own_sq = jnp.sum(combined * combined, axis=1, keepdims=True)
    eye = lax.broadcasted_iota(I32, (blk, blk), 0) == lax.broadcasted_iota(I32, (blk, blk), 1)
    flat = jnp.sum(jnp.where(eye, jnp.broadcast_to(own_sq, (blk, blk)), 0.0), axis=0, keepdims=True)
    squares[x] = jnp.broadcast_to(jnp.concatenate([flat, flat], axis=1), squares.shape[1:])

    def q_copy(q):
        return pltpu.make_async_remote_copy(
            squares.at[x], squares.at[x], out_sem.at[8], q_recv.at[0],
            device_id={"tp": wrap(x + q, tp)}, device_id_type=MESH)

    for q in range(1, tp):
        q_copy(q).start()

    def amount(units, most):
        b = max(d for d in range(1, most + 1) if units % d == 0)
        return units // b, b

    a, b = amount(2 * steps - 1, 4)
    whole(tok.at[0:a, :, 0:b * blk, :], out_sem.at[0]).wait()
    whole(tab.at[0:a, 0:b], out_sem.at[1]).wait()
    a, b = amount(2 * steps, 4)
    whole(tok.at[0:a, :, 0:b * blk, :], out_sem.at[2]).wait()
    whole(tab.at[0:a, 0:b], out_sem.at[3]).wait()
    if XS:
        whole(rows.at[0:steps, :, 0:XS * share], out_sem.at[4]).wait()
    whole(part.at[0:steps, 0:tp - 1], out_sem.at[5]).wait()
    whole(results.at[0:ep - 1], out_sem.at[7]).wait()
    whole(squares.at[0:tp - 1], out_sem.at[8]).wait()
    whole(squares.at[0:tp - 1], q_recv.at[0]).wait()
    everyone = jnp.sum(squares[...], axis=0)[0:1, 0:blk]
    column = jnp.sum(jnp.where(eye, jnp.broadcast_to(everyone, (blk, blk)), 0.0), axis=1, keepdims=True)
    scale = lax.rsqrt(column / (tp * share) + EPS)
    out[...] = (combined * scale * final_in[...]).astype(out.dtype)


def solution(mesh):
    ep, tp = mesh.shape["ep"], mesh.shape["tp"]

    def per_device(tokens, norm_gain, routes, route_weights, w_gate, w_up, w_down, final_gain):
        blk, features = tokens.shape
        cap = max(2, min(blk, 2 * blk * TOP_K // ep))
        share = features // tp
        slots = ep // CORES // 2 + 1
        hl = tp // 2
        zs = tp - XS
        dma = pltpu.SemaphoreType.DMA
        vmem = pltpu.VMEM
        return pl.pallas_call(
            functools.partial(kernel, ep, tp, cap),
            out_shape=jax.ShapeDtypeStruct((blk, share), BF16),
            in_specs=[pl.BlockSpec(memory_space=pl.ANY)] * 8,
            out_specs=pl.BlockSpec(memory_space=pltpu.VMEM),
            scratch_shapes=[
                vmem((slots, zs, 4 * blk, share), BF16),
                vmem((slots, 4, ep, 2 * blk), BF16),
                vmem((slots, 4 * cap, features), BF16),
                vmem((slots, tp, 4 * cap, share), BF16),
                vmem((slots, hl, 2, 4 * cap, share), BF16),
                vmem((slots, 4, cap, share), BF16),
                vmem((ep, cap, share), BF16),
                vmem((CORES, cap, share), BF16),
                vmem((tp, 8, 2 * blk), F32),
                vmem((tp, blk, share), BF16),
                vmem((tp, 1, share), F32),
                vmem((TOP_K, blk), I32),
                vmem((TOP_K, blk), F32),
                vmem((features, 2 * share), BF16),
                vmem((tp, share, share), BF16),
                vmem((1, share), F32),
                vmem((blk, ep * cap), BF16),
                vmem((blk, ep * cap), BF16),
                vmem((blk, CORES * cap), BF16),
                vmem((blk, CORES * cap), BF16),
                dma((7,)), dma((9,)),
                dma((slots - 1, len(PIECES) + 1)), dma((slots, 2)), dma((slots,)), dma((slots, hl)), dma((2,)), dma((1,)),
            ],
            compiler_params=pltpu.CompilerParams(
                collective_id=0, has_side_effects=True, vmem_limit_bytes=56 * 1024 * 1024),
        )(tokens, norm_gain.reshape(1, features), routes.T, route_weights.T, w_gate, w_up, w_down,
          final_gain.reshape(1, share))

    placed = (
        P(("grp", "ep"), None),
        P(),
        P(("grp", "ep"), None),
        P(("grp", "ep"), None),
        P("ep", None, "tp"),
        P("ep", None, "tp"),
        P("ep", "tp", None),
        P("tp"),
    )
    return jax.shard_map(
        per_device, mesh=mesh, in_specs=placed, out_specs=P(("grp", "ep"), "tp"), check_vma=False
    )
```
